32 devices in a mesh: pp: 4 (over z), fs: 4 (over y, x), tp: 2 (over core).
Axes of the slice: x: 2, y: 2, z: 4, core: 2. Of those that a mesh axis runs over, the one named last changes fastest.
Arguments:
- tokens: bfloat16 [4, 512, 1024], P('pp', 'fs', 'tp'), parts along dimension 1, may hold values from -640 to 640
- query_matrix: bfloat16 [4, 1024, 1024], P('pp', None, 'tp'), may hold values from -0.1875 to 0.1875
- key_matrix: bfloat16 [4, 1024, 1024], P('pp', None, 'tp'), may hold values from -0.1875 to 0.1875
- value_matrix: bfloat16 [4, 1024, 1024], P('pp', None, 'tp'), may hold values from -0.1875 to 0.1875
- output_gate_weight: bfloat16 [4, 1024, 1024], P('pp', None, 'tp'), may hold values from -0.1875 to 0.1875
- strength_weight: bfloat16 [4, 1024, 8], P('pp', None, 'tp'), may hold values from -0.1875 to 0.1875
- decay_input_weight: bfloat16 [4, 1024, 8], P('pp', None, 'tp'), may hold values from -0.1875 to 0.1875
- decay_scale_table: float32 [4, 8], P('pp', 'tp'), may hold values from 0.00078125 to 0.234375
- log_spike_decay: float32 [4, 128, 8], P('pp', None, 'tp'), may hold values from -2.1 to 0
- head_norm_gain: float32 [4, 1024], P('pp', 'tp'), may hold values from 0.1 to 1.9
- closing_norm_gain: float32 [1024], P('tp'), may hold values from 0.1 to 1.9
Outputs:
- normalized: bfloat16 [4, 512, 1024], P('pp', 'fs', 'tp'), parts along dimension 1
The draws below stay inside these ranges and needn't reach their ends.
There are 4 independent parts, one for each index of `fs`. The reference program is written for one: setup_inputs(seed, part) draws one part's arguments, and reference() takes and returns one part's arrays. A program takes and returns all parts, laid end to end along the dimension named above; an argument that names none is the same for every part. Nothing has to cross between parts.
All inputs are finite; a program needn't handle non-finite values.
Results may differ from the reference program's by a relative error of at most 0.012.
Values may be sent and summed in bfloat16 or wider, within the bound.
A program may use at most 64 MiB of HBM per device.

```python
import math
from functools import partial
import jax
import jax.numpy as jnp
from jax import lax

D = 1024
HEAD_TOTAL = 8
HEAD_DIM = 128
BLOCK = 64
SEQUENCE_LENGTH = 128
LAYER_TOTAL = 4
MICRO = 4


spike_count = 3


def draw_tokens(key, part):
    base_key, row_key = jax.random.split(jax.random.fold_in(key, 17), 2)
    column_ramp = jnp.exp(math.log(10.0) * jnp.arange(D, dtype=jnp.float32) / (D - 1))
    base_values = jnp.clip(jax.random.normal(base_key, (MICRO, SEQUENCE_LENGTH, D), jnp.float32), -4.0, 4.0)
    row_scale = jnp.exp(jax.random.uniform(row_key, (MICRO, SEQUENCE_LENGTH, 1), jnp.float32, 0.0, math.log(10.0)))
    return (base_values * row_scale * column_ramp).astype(jnp.bfloat16)


def draw_decay_scale_table(key, part):
    lower_rate = 0.3 / SEQUENCE_LENGTH
    upper_rate = 30.0 / SEQUENCE_LENGTH
    logged = jax.random.uniform(jax.random.fold_in(key, 23), (LAYER_TOTAL, HEAD_TOTAL), jnp.float32, math.log(lower_rate), math.log(upper_rate))
    return jnp.exp(logged)


def draw_log_spike_decay(key, part):
    position_random_key, layer_random_key = jax.random.split(jax.random.fold_in(key, 29))
    position_indices = jax.random.randint(position_random_key, (LAYER_TOTAL, spike_count, HEAD_TOTAL), 0, SEQUENCE_LENGTH)
    layer_indices = jnp.log(jax.random.uniform(layer_random_key, (LAYER_TOTAL, spike_count, HEAD_TOTAL), jnp.float32, 0.5, 0.8))
    hit_mask = (position_indices[:, :, None, :] == jnp.arange(SEQUENCE_LENGTH)[None, None, :, None]).astype(jnp.float32)
    return jnp.sum(hit_mask * layer_indices[:, :, None, :], axis=1)


def shard_levels(own_key, extent, cuts, least, top_value):
    level = 1.0
    for dim, shards_of in cuts:
        steps = jax.random.uniform(jax.random.fold_in(jax.random.fold_in(own_key, 6), dim), (shards_of,), jnp.float32, least / len(cuts), top_value / len(cuts))
        level = level * jnp.repeat(jnp.exp(steps), extent[dim] // shards_of).reshape((-1,) + (1,) * (len(extent) - 1 - dim))
    return level


def gaussian(own_key, extent, deviation, reach, shards=(), kind=jnp.bfloat16):
    factor_of = shard_levels(own_key, extent, shards, -0.22, 0.18) if shards else 1.0
    drawn = jax.random.normal(own_key, extent, jnp.float32) * deviation * factor_of
    return jnp.minimum(jnp.maximum(drawn, -reach), reach).astype(kind)


def setup_inputs(seed: int = 0, part: int = 0) -> dict:
    splits = jax.random.split(jax.random.key(seed), 12)
    part_splits = jax.random.split(jax.random.fold_in(splits[11], part), 12)
    return {
        "tokens": draw_tokens(jax.random.fold_in(jax.random.fold_in(splits[11], part), 71), part),
        "query_matrix": gaussian(splits[1], (LAYER_TOTAL, D, HEAD_TOTAL * HEAD_DIM), D ** -0.5, 0.1875, ((0, 4), (2, 2))),
        "key_matrix": gaussian(splits[2], (LAYER_TOTAL, D, HEAD_TOTAL * HEAD_DIM), D ** -0.5, 0.1875, ((0, 4), (2, 2))),
        "value_matrix": gaussian(splits[3], (LAYER_TOTAL, D, HEAD_TOTAL * HEAD_DIM), D ** -0.5, 0.1875, ((0, 4), (2, 2))),
        "output_gate_weight": gaussian(splits[4], (LAYER_TOTAL, D, HEAD_TOTAL * HEAD_DIM), D ** -0.5, 0.1875, ((0, 4), (2, 2))),
        "strength_weight": gaussian(splits[5], (LAYER_TOTAL, D, HEAD_TOTAL), D ** -0.5, 0.1875, ((0, 4), (2, 2))),
        "decay_input_weight": gaussian(splits[6], (LAYER_TOTAL, D, HEAD_TOTAL), D ** -0.5, 0.1875, ((0, 4), (2, 2))),
        "decay_scale_table": draw_decay_scale_table(jax.random.fold_in(splits[11], 71), part),
        "log_spike_decay": draw_log_spike_decay(jax.random.fold_in(splits[11], 71), part),
        "head_norm_gain": jnp.clip(1.0 + 0.18 * jax.random.normal(splits[9], (LAYER_TOTAL, HEAD_TOTAL * HEAD_DIM), jnp.float32), 0.1, 1.9),
        "closing_norm_gain": jnp.clip(1.0 + 0.18 * jax.random.normal(splits[10], (D,), jnp.float32), 0.1, 1.9),
    }


epsilon = 1e-06

def delta_rule(queries, keys_unit, values, beta_gate, decay_logarithm):
    length, head_count, head_width = queries.shape
    value_width = values.shape[-1]
    num_blocks = length // BLOCK
    best_precision = lax.Precision.HIGHEST

    def to_blocks(tensor):
        return tensor.reshape(num_blocks, BLOCK, head_count, -1).transpose(2, 0, 1, 3)
    query_b = to_blocks(queries)
    keys_b = to_blocks(keys_unit)
    values_b = to_blocks(values)
    beta_b = beta_gate.reshape(num_blocks, BLOCK, head_count).transpose(2, 0, 1)
    decay_b = decay_logarithm.reshape(num_blocks, BLOCK, head_count).transpose(2, 0, 1)
    cumulative = jnp.cumsum(decay_b, axis=-1)
    row_ids = lax.broadcasted_iota(jnp.int32, (BLOCK, BLOCK), 0)
    col_ids = lax.broadcasted_iota(jnp.int32, (BLOCK, BLOCK), 1)
    within = jnp.where(row_ids >= col_ids, cumulative[..., :, None] - cumulative[..., None, :], -jnp.inf)
    weights = jnp.exp(within)
    keys_beta = keys_b * beta_b[..., None]
    self_term = jnp.where(row_ids > col_ids, jnp.einsum('hnik,hnjk->hnij', keys_beta, keys_b, precision=best_precision) * weights, 0.0)
    system = self_term + jnp.eye(BLOCK, dtype=self_term.dtype)
    right_side = jnp.concatenate([values_b * beta_b[..., None], keys_beta * jnp.exp(cumulative)[..., None]], axis=-1)
    solved = jax.scipy.linalg.solve_triangular(system, right_side, lower=True, unit_diagonal=True)
    update = solved[..., :value_width]
    correct = solved[..., value_width:]
    scores = jnp.einsum('hnik,hnjk->hnij', query_b, keys_b, precision=best_precision) * weights
    query_dec = query_b * jnp.exp(cumulative)[..., None]
    keys_dec = keys_b * jnp.exp(cumulative[..., -1:] - cumulative)[..., None]
    block_decay = jnp.exp(cumulative[..., -1])

    def advance(state_matrix, inputs):
        state_update, correction_term, normed_queries, normed_keys, attention_scores, decay_factor = inputs
        new_state = state_update - jnp.einsum('rna,raq->rnq', correction_term, state_matrix, precision=best_precision)
        normed_output = jnp.einsum('rna,raq->rnq', normed_queries, state_matrix, precision=best_precision) + jnp.einsum('pak,pkr->par', attention_scores, new_state, precision=best_precision)
        state_matrix = state_matrix * decay_factor[:, None, None] + jnp.einsum('fni,fnl->fil', normed_keys, new_state, precision=best_precision)
        return (state_matrix, normed_output)
    sequence_in = tuple((jnp.moveaxis(tensor, 1, 0) for tensor in (update, correct, query_dec, keys_dec, scores, block_decay)))
    initial_state = jnp.zeros((head_count, head_width, value_width), jnp.float32)
    final_state, outputs = lax.scan(advance, initial_state, sequence_in)
    return outputs.transpose(0, 2, 1, 3).reshape(length, head_count, value_width)

def merge_head_outputs(query_projected, key_projected, value_projected, gate_logits, strength_logits, decay_logits, decay_speed, spike_log_values, gain_vector):
    length = query_projected.shape[0]
    head_count = strength_logits.shape[-1]
    head_width = query_projected.shape[1] // head_count

    def normalize(projected):
        activated = jax.nn.silu(projected).reshape(length, head_count, -1)
        return activated * lax.rsqrt(lax.optimization_barrier(jnp.sum(activated * activated, axis=-1, keepdims=True)) + epsilon)
    queries = normalize(query_projected) * head_width ** (-0.5)
    keys_unit = normalize(key_projected)
    values = jax.nn.silu(value_projected).reshape(length, head_count, -1)
    beta_gate = jax.nn.sigmoid(strength_logits)
    decay_logarithm = -decay_speed[None, :] * jax.nn.softplus(decay_logits) + spike_log_values
    mixed_out = delta_rule(queries, keys_unit, values, beta_gate, decay_logarithm)
    mixed_out = mixed_out * lax.rsqrt(lax.optimization_barrier(jnp.mean(mixed_out * mixed_out, axis=-1, keepdims=True)) + epsilon) * gain_vector.reshape(head_count, -1) * jax.nn.silu(gate_logits).reshape(length, head_count, -1)
    return mixed_out.reshape(length, -1).astype(jnp.bfloat16)

def reference(tokens, query_matrix, key_matrix, value_matrix, output_gate_weight, strength_weight, decay_input_weight, decay_scale_table, log_spike_decay, head_norm_gain, closing_norm_gain):
    hidden = tokens
    for layer_number in range(LAYER_TOTAL):
        flat_rows = hidden.reshape(-1, D)
        square = flat_rows.astype(jnp.float32)
        inv_rms = lax.rsqrt(lax.optimization_barrier(jnp.mean(square * square, axis=-1, keepdims=True)) + epsilon)
        projected = [(jnp.dot(flat_rows.astype(jnp.float32), matrix[layer_number].astype(jnp.float32), preferred_element_type=jnp.float32) * inv_rms).reshape(MICRO, SEQUENCE_LENGTH, -1) for matrix in (query_matrix, key_matrix, value_matrix, output_gate_weight, strength_weight, decay_input_weight)]
        token_mixer = partial(merge_head_outputs, decay_speed=decay_scale_table[layer_number], spike_log_values=log_spike_decay[layer_number], gain_vector=head_norm_gain[layer_number])
        mixed_out = jax.vmap(token_mixer)(projected[0], projected[1], projected[2], projected[3], projected[4], projected[5])
        hidden = (hidden.astype(jnp.float32) + mixed_out.astype(jnp.float32)).astype(jnp.bfloat16)
    square = hidden.astype(jnp.float32)
    inv_rms = lax.rsqrt(lax.optimization_barrier(jnp.mean(square * square, axis=-1, keepdims=True)) + epsilon)
    return (square * inv_rms * closing_norm_gain).astype(jnp.bfloat16)
```

```python
import functools
import jax
import jax.numpy as jnp
from jax import lax
from jax.experimental import pallas as pl
from jax.experimental.pallas import tpu as pltpu
from jax.sharding import PartitionSpec as P

epsilon = 1e-06
F32 = jnp.float32
BF16 = jnp.bfloat16
MESH = pl.DeviceIdType.MESH
NT = (((1,), (1,)), ((), ()))


def silu(a):
    return a * (0.5 + 0.5 * jnp.tanh(0.5 * a))


def dot(a, b):
    return jnp.dot(a.astype(BF16), b.astype(BF16), preferred_element_type=F32)


def stack_kernel(
    stages,
    group,
    size,
    tokens,
    query_hbm,
    key_hbm,
    value_hbm,
    gate_hbm,
    strength_hbm,
    decay_in_hbm,
    decay_speed_hbm,
    spike_hbm,
    gain_hbm,
    closing_hbm,
    out,
    strength,
    decay_in,
    decay_speed,
    spike,
    gain,
    closing_gain,
    weights,
    acc,
    squares_own,
    beta_own,
    decay_own,
    decay_wide,
    speed_wide,
    spike_wide,
    xin,
    xout,
    yin,
    past_key,
    past_value,
    past_fade,
    part_mine,
    part_other,
    w_sem,
    small_sem,
    token_sem,
    go_sem,
    in_sem,
    entry_sem,
    fwd_send,
    fwd_recv,
    out_send,
    y_recv,
    part_send,
    part_recv,
):
    stage = lax.axis_index("pp")
    core = lax.axis_index("tp")
    last = stages - 1
    length, half = tokens.shape
    heads = xout.shape[1]
    width = half // heads
    model_width = group * half
    others = range(1, group)
    spans = [slice(start, start + size) for start in range(0, length, size)]

    def peer(d):
        return lax.rem(core + d, group)

    barrier = pltpu.get_barrier_semaphore()
    for d in range(1, stages):
        pl.semaphore_signal(
            barrier, inc=1, device_id={"pp": lax.rem(stage + d, stages)}, device_id_type=MESH
        )
    for d in others:
        pl.semaphore_signal(barrier, inc=1, device_id={"tp": peer(d)}, device_id_type=MESH)

    def token_copy(h, target):
        return pltpu.make_async_copy(
            tokens.at[:, h * width : (h + 1) * width], target, token_sem.at[h]
        )

    @pl.when(stage == 0)
    def _():
        for h in range(heads):
            token_copy(h, xin.at[0, core * heads + h]).start()

    @pl.when(stage > 0)
    def _():
        for h in range(heads):
            token_copy(h, xout.at[stages, h]).start()

    small_loads = [
        pltpu.make_async_copy(a, b, small_sem.at[i])
        for i, (a, b) in enumerate(
            (
                (strength_hbm, strength),
                (decay_in_hbm, decay_in),
                (decay_speed_hbm, decay_speed),
                (spike_hbm, spike),
                (gain_hbm, gain),
                (closing_hbm, closing_gain),
            )
        )
    ]
    for load in small_loads:
        load.start()
    loads = [
        pltpu.make_async_copy(ref, weights.at[i], w_sem.at[i])
        for i, ref in enumerate((key_hbm, query_hbm, value_hbm, gate_hbm))
    ]
    for load in loads:
        load.start()

    pl.semaphore_wait(barrier, stages + group - 2)

    def entry_copy(h, span):
        return pltpu.make_async_remote_copy(
            src_ref=xout.at[stages, h, span],
            dst_ref=xin.at[stage, core * heads + h, span],
            send_sem=entry_sem.at[span.start // size, h],
            recv_sem=in_sem.at[stage, span.start // size, h],
            device_id={"pp": 0},
            device_id_type=MESH,
        )

    def next_copy(m, h, span):
        return pltpu.make_async_remote_copy(
            src_ref=xout.at[m, h, span],
            dst_ref=xin.at[m, core * heads + h, span],
            send_sem=out_send.at[m, span.start // size, h],
            recv_sem=in_sem.at[m, span.start // size, h],
            device_id={"pp": lax.rem(stage + 1, stages)},
            device_id_type=MESH,
        )

    def exit_copy(m, h, span):
        return pltpu.make_async_remote_copy(
            src_ref=xout.at[m, h, span],
            dst_ref=yin.at[h, span],
            send_sem=out_send.at[m, span.start // size, h],
            recv_sem=y_recv.at[span.start // size, h],
            device_id={"pp": m},
            device_id_type=MESH,
        )

    def forward_copy(m, d, h, span):
        return pltpu.make_async_remote_copy(
            src_ref=xin.at[m, core * heads + h, span],
            dst_ref=xin.at[m, core * heads + h, span],
            send_sem=fwd_send.at[m, d - 1, span.start // size, h],
            recv_sem=fwd_recv.at[m, d - 1, span.start // size, h],
            device_id={"tp": peer(d)},
            device_id_type=MESH,
        )

    @pl.when(stage == 0)
    def _():
        for h in range(heads):
            token_copy(h, xin.at[0, core * heads + h]).wait()

    early = max(heads - 2, 0)

    @pl.when(stage > 0)
    def _():
        for h in range(heads):
            token_copy(h, xout.at[stages, h]).wait()

        @pl.when(stage > 1)
        def _():
            pl.semaphore_wait(go_sem, 1)

        for span in spans:
            for h in range(heads):
                entry_copy(h, span).start()
        entry_copy(early, spans[-1]).wait_send()

        @pl.when(stage < last)
        def _():
            pl.semaphore_signal(
                go_sem, inc=1, device_id={"pp": lax.rem(stage + 1, stages)}, device_id_type=MESH
            )

    for load in small_loads:
        load.wait()
    side = min(length // size, heads)
    groups = heads // side
    lanes = side * size
    block = min(16, size)
    pieces = size // block
    every = range(groups)
    spike_columns = jnp.concatenate(
        [spike[...], jnp.zeros((length - heads, length), F32)], axis=0
    ).T
    for g in every:
        for p in range(side):
            h = g + p * groups
            at = slice(g * lanes + p * size, g * lanes + (p + 1) * size)
            speed_wide[:, at] = jnp.broadcast_to(decay_speed[:, h : h + 1], (1, size))
        spread = jnp.broadcast_to(spike_columns[:, g : g + 1], (length, lanes))
        for p in range(1, side):
            h = g + p * groups
            lane = lax.broadcasted_iota(jnp.int32, (length, lanes), 1)
            other = jnp.broadcast_to(spike_columns[:, h : h + 1], (length, lanes))
            spread = jnp.where(lane >= p * size, other, spread)
        spike_wide[:, g * lanes : (g + 1) * lanes] = spread
    tile = min(256, model_width)
    same = lax.broadcasted_iota(jnp.int32, (tile, tile), 0) == lax.broadcasted_iota(
        jnp.int32, (tile, tile), 1
    )
    identity = jnp.where(same, 1.0, 0.0).astype(BF16)
    for start in range(0, model_width, tile):
        part = decay_in[:heads, start : start + tile].astype(F32)
        wide = jnp.concatenate(
            [
                jnp.broadcast_to(part[g + p * groups : g + p * groups + 1], (size, tile))
                for g in every
                for p in range(side)
            ],
            axis=0,
        ).astype(BF16)
        decay_wide[start : start + tile, :] = lax.dot_general(
            identity, wide, NT, preferred_element_type=F32
        ).astype(BF16)

    def gather(m, which, span):
        return jnp.concatenate([xin[m, which * heads + h, span] for h in range(heads)], axis=1)

    def glance(x, which):
        own = pl.ds(pl.multiple_of(which * half, half), half)
        wide = x.astype(F32)
        squares = jnp.sum(wide * wide, axis=1, keepdims=True)
        decay = dot(x, decay_wide[own, :])
        beta = lax.dot_general(x, strength[:, own], NT, preferred_element_type=F32)
        return squares, decay, beta[:, :heads]

    def project(x, which):
        own = pl.ds(pl.multiple_of(which * half, half), half)
        return [dot(x, weights[i, own, :]) for i in range(4)]

    def begin(m, span):
        x = gather(m, core, span)
        squares, decay, beta = glance(x, core)
        squares_own[span] = jnp.broadcast_to(squares, (size, width))
        decay_own[span] = decay
        beta_own[span] = beta
        for i, a in enumerate(project(x, core)):
            acc[i, span] = a

    def chunk(m, span, keep, use, between):
        squares = squares_own[span, :1]
        decay = decay_own[span]
        beta = beta_own[span]
        for d in others:
            for h in range(heads):
                forward_copy(m, d, h, span).wait_recv()
            source = peer(group - d)
            x = gather(m, source, span)
            squares_other, decay_other, beta_other = glance(x, source)
            squares = squares + squares_other
            decay = decay + decay_other
            beta = beta + beta_other
            for h in range(heads):
                forward_copy(m, d, h, span).wait_send()
            mats = project(x, source)
            if d < group - 1:
                for i in range(4):
                    acc[i, span] += mats[i]
        inv_rms = lax.rsqrt(squares / model_width + epsilon)

        row = lax.broadcasted_iota(jnp.int32, (size, lanes), 0)
        lane = lax.broadcasted_iota(jnp.int32, (size, lanes), 1)
        column = lane % size
        band = (lax.broadcasted_iota(jnp.int32, (8, lanes), 1) % size) // block

        beta = 1.0 / (1.0 + jnp.exp(-beta * inv_rms))
        pre = decay * inv_rms
        softplus = jnp.maximum(pre, 0.0) + jnp.log(1.0 + jnp.exp(-jnp.abs(pre)))
        log_decay = spike_wide[span, :] - speed_wide[...] * softplus
        lower = jnp.where(
            lax.broadcasted_iota(jnp.int32, (size, size), 0)
            >= lax.broadcasted_iota(jnp.int32, (size, size), 1),
            1.0,
            0.0,
        ).astype(BF16)
        high = log_decay.astype(BF16)
        rest = log_decay - high.astype(F32)
        after = jnp.concatenate([row > column] * groups, axis=1)

        def total(mask):
            picked = (jnp.where(after, a.astype(F32), 0.0) if mask else a for a in (high, rest))
            return sum(dot(lower, a) for a in picked)

        since = total(True)
        if use:
            whole = total(False)

        def packed(which, g):
            return jnp.concatenate([which[g + p * groups] for p in range(side)], axis=1)

        def apart(which, g):
            empty = jnp.zeros_like(which[0])
            return jnp.concatenate(
                [
                    jnp.concatenate(
                        [which[g + p * groups] if s == p else empty for s in range(side)], axis=1
                    )
                    for p in range(side)
                ],
                axis=0,
            )

        def stacked(square):
            if side == 1:
                return square
            return jnp.concatenate(
                [jnp.where(lane // size == p, square, jnp.zeros_like(square)) for p in range(side)],
                axis=0,
            )

        def columns(i, h):
            part = slice(h * width, (h + 1) * width)
            return (acc[i, span, part] + mats[i][:, part]) * inv_rms

        def norm(a):
            return lax.rsqrt(jnp.sum(a * a, axis=1, keepdims=True) + epsilon)

        keys = [silu(columns(0, h)) for h in range(heads)]
        rounded_keys = [a.astype(BF16) for a in keys]
        queries = [silu(columns(1, h)) for h in range(heads)]
        rounded_queries = [a.astype(BF16) for a in queries]
        gram = []
        for g in every:
            left = jnp.concatenate([packed(rounded_keys, g), packed(rounded_queries, g)], axis=0)
            gram.append(
                lax.dot_general(left, apart(rounded_keys, g), NT, preferred_element_type=F32)
            )
        key_scale = [norm(a) for a in keys]
        query_scale = [norm(a) * width ** (-0.5) for a in queries]
        force = [beta[:, h : h + 1] * key_scale[h] for h in range(heads)]
        weight = [force[h] * key_scale[h] for h in range(heads)]
        values = [silu(columns(2, h)) * force[h] for h in range(heads)]

        def stretch(parts, g):
            out = jnp.broadcast_to(parts[g], (size, lanes))
            for p in range(1, side):
                out = jnp.where(
                    lane >= p * size, jnp.broadcast_to(parts[g + p * groups], (size, lanes)), out
                )
            return out

        def section(wide, g):
            return wide[:, g * lanes : (g + 1) * lanes]

        decayed = [jnp.where(row >= column, jnp.exp(section(since, g)), 0.0) for g in every]
        scale = [stretch(weight, g) for g in every]
        system = [
            jnp.where(row > column, gram[g][:size] * decayed[g], 0.0) * scale[g] for g in every
        ]
        scores = [(gram[g][size:] * decayed[g]).astype(BF16) for g in every]

        before = None
        if use:
            past_keys = [past_key[h] for h in range(heads)]
            past_values = [past_value[h] for h in range(heads)]
            before = []
            for g in every:
                left = jnp.concatenate(
                    [packed(rounded_keys, g), packed(rounded_queries, g)], axis=0
                )
                cross = lax.dot_general(left, apart(past_keys, g), NT, preferred_element_type=F32)
                fade = jnp.exp(section(whole, g) + past_fade[g : g + 1, :])
                cross = (cross * jnp.concatenate([fade, fade], axis=0)).astype(BF16)
                before.append(
                    jnp.dot(cross, apart(past_values, g), preferred_element_type=F32)
                )
            for g in every:
                for p in range(side):
                    h = g + p * groups
                    part = slice(p * width, (p + 1) * width)
                    values[h] = values[h] - weight[h] * before[g][:size, part]

        tiles = block // 8
        inverse = []
        for g in every:
            compact = []
            for t in range(tiles):
                tile = system[g][t * 8 : t * 8 + 8]
                for r in range(1, pieces):
                    at = r * block + t * 8
                    tile = jnp.where(band == r, system[g][at : at + 8], tile)
                compact.append(tile)
            inner = lax.broadcasted_iota(jnp.int32, (8, lanes), 1) % block
            down_rows = lax.broadcasted_iota(jnp.int32, (8, lanes), 0)
            solved = [
                jnp.where(down_rows + t * 8 == inner, 1.0, 0.0).astype(F32) for t in range(tiles)
            ]
            start_of = lax.broadcasted_iota(jnp.int32, (8, lanes), 1) - inner
            for j in range(block - 1):
                source = jnp.broadcast_to(
                    solved[j // 8][j % 8 : j % 8 + 1, :], (8, lanes)
                )
                for t in range((j + 1) // 8, tiles):
                    factor = jnp.take_along_axis(
                        compact[t], start_of + j, axis=1, mode="promise_in_bounds"
                    )
                    solved[t] = solved[t] - factor * source
            inverse.append(
                jnp.concatenate(
                    [
                        jnp.where(band == r, solved[t], 0.0).astype(F32)
                        for r in range(pieces)
                        for t in range(tiles)
                    ],
                    axis=0,
                ).astype(BF16)
            )
        between()
        update = [dot(inverse[g], apart([a.astype(BF16) for a in values], g)) for g in every]

        def split(wide):
            return [
                wide[h % groups][:, (h // groups) * width : (h // groups + 1) * width].astype(BF16)
                for h in range(heads)
            ]

        if pieces > 1:
            outside = row // block != column // block
            chain = [
                dot(inverse[g], stacked(jnp.where(outside, system[g], 0.0).astype(BF16)))
                for g in every
            ]
            sign = -1.0
            done = 1
            while done < pieces:
                rounded = [chain[g].astype(BF16) for g in every]
                current = split(update)
                update = [
                    update[g] + sign * dot(rounded[g], apart(current, g)) for g in every
                ]
                done *= 2
                sign = 1.0
                if done < pieces:
                    chain = [dot(rounded[g], stacked(rounded[g])) for g in every]
        final = split(update)
        mixed = [dot(scores[g], apart(final, g)) for g in every]
        if use:
            mixed = [mixed[g] + before[g][size:] for g in every]
        for h in range(heads):
            part = slice((h // groups) * width, (h // groups + 1) * width)
            raw = mixed[h % groups][:, part]
            gate = silu(columns(3, h)) * gain[:, h * width : (h + 1) * width]
            mean = jnp.mean(raw * raw, axis=1, keepdims=True)
            unit = query_scale[h]
            head_out = raw * (unit * lax.rsqrt(unit * unit * mean + epsilon)) * gate
            x = xin[m, core * heads + h, span].astype(F32)
            xout[m, h, span] = (x + head_out.astype(BF16).astype(F32)).astype(BF16)
        if keep:
            for h in range(heads):
                past_key[h] = rounded_keys[h]
                past_value[h] = final[h]
            for g in every:
                past_fade[g : g + 1, :] = section(since, g)[size - 1 : size, :]

    def arrive(m, span):
        for h in range(heads):
            next_copy(m, h, span).wait_recv()
            for d in others:
                forward_copy(m, d, h, span).start()

    def enter(span):
        @pl.when(stage > 0)
        def _():
            arrive(0, span)

        @pl.when(stage == 0)
        def _():
            for h in range(heads):
                for d in others:
                    forward_copy(0, d, h, span).start()

    def leave(m, span):
        @pl.when(stage < last)
        def _():
            for h in range(heads):
                next_copy(m, h, span).start()

        @pl.when((stage == last) & (m < last))
        def _():
            for h in range(heads):
                exit_copy(m, h, span).start()

    def step(m, _):
        for i, span in enumerate(spans):

            def between(i=i):
                if i + 1 < len(spans):
                    following, ahead = m, spans[i + 1]

                    @pl.when((stage > 0) | (m > 0))
                    def _():
                        arrive(following, ahead)

                else:
                    following, ahead = lax.rem(m + 1, stages), spans[0]

                    @pl.when(m < last)
                    def _():
                        arrive(following, ahead)

                begin(following, ahead)

            chunk(m, span, keep=i + 1 < len(spans), use=i > 0, between=between)
            leave(m, span)
        return 0

    enter(spans[0])
    for load in loads:
        load.wait()
    begin(0, spans[0])

    @pl.when(stage == 0)
    def _():
        for span in spans[1:]:
            for h in range(heads):
                for d in others:
                    forward_copy(0, d, h, span).start()

    lax.fori_loop(0, stages, step, 0)

    @pl.when(stage == last)
    def _():
        for h in range(heads):
            yin[h] = xout[last, h]

    @pl.when(stage < last)
    def _():
        for span in spans:
            for h in range(heads):
                exit_copy(0, h, span).wait_recv()

    final = [yin[h].astype(F32) for h in range(heads)]
    total = sum(jnp.sum(a * a, axis=1, keepdims=True) for a in final)
    part_mine[...] = jnp.broadcast_to(total, part_mine.shape)
    part_copies = [
        pltpu.make_async_remote_copy(
            src_ref=part_mine,
            dst_ref=part_other.at[d - 1],
            send_sem=part_send.at[d - 1],
            recv_sem=part_recv.at[d - 1],
            device_id={"tp": peer(d)},
            device_id_type=MESH,
        )
        for d in others
    ]
    for copy in part_copies:
        copy.start()

    @pl.when(stage > 0)
    def _():
        for span in spans:
            for h in range(heads):
                if h != early or span is not spans[-1]:
                    entry_copy(h, span).wait_send()

    def drain(m, _):
        @pl.when((stage < last) | (m < last))
        def _():
            for span in spans:
                for h in range(heads):
                    next_copy(m, h, span).wait_send()

        return 0

    lax.fori_loop(0, stages, drain, 0)
    total = part_mine[...]
    for copy in part_copies:
        copy.wait()
    for d in others:
        total = total + part_other[d - 1]
    inv_rms = lax.rsqrt(total / model_width + epsilon)
    for h in range(heads):
        part = slice(h * width, (h + 1) * width)
        out[:, part] = (final[h] * inv_rms * closing_gain[:, part]).astype(BF16)


def on_device(
    stages,
    group,
    tokens,
    query_matrix,
    key_matrix,
    value_matrix,
    output_gate_weight,
    strength_weight,
    decay_input_weight,
    decay_scale_table,
    log_spike_decay,
    head_norm_gain,
    closing_norm_gain,
):
    _, length, half = tokens.shape
    heads = strength_weight.shape[-1]
    width = half // heads
    parts = 2 if heads % 2 == 0 else 1
    size = length // parts

    def rows_of(weight):
        return jnp.pad(weight[0].T, ((0, 1), (0, 0))) if heads == 1 else weight[0].T

    vmem = pl.BlockSpec(memory_space=pltpu.VMEM)
    anywhere = pl.BlockSpec(memory_space=pltpu.HBM)
    dma = pltpu.SemaphoreType.DMA
    result = pl.pallas_call(
        functools.partial(stack_kernel, stages, group, size),
        out_shape=pltpu.VMEM((length, half), BF16),
        in_specs=[anywhere] * 11,
        out_specs=vmem,
        scratch_shapes=[
            pltpu.VMEM((max(heads, 2), group * half), BF16),
            pltpu.VMEM((max(heads, 2), group * half), BF16),
            pltpu.VMEM((1, heads), F32),
            pltpu.VMEM((heads, length), F32),
            pltpu.VMEM((1, half), F32),
            pltpu.VMEM((1, half), F32),
            pltpu.VMEM((4, group * half, half), BF16),
            pltpu.VMEM((4, length, half), F32),
            pltpu.VMEM((length, width), F32),
            pltpu.VMEM((length, heads), F32),
            pltpu.VMEM((length, heads * size), F32),
            pltpu.VMEM((group * half, heads * size), BF16),
            pltpu.VMEM((1, heads * size), F32),
            pltpu.VMEM((length, heads * size), F32),
            pltpu.VMEM((stages, group * heads, length, width), BF16),
            pltpu.VMEM((stages + 1, heads, length, width), BF16),
            pltpu.VMEM((heads, length, width), BF16),
            pltpu.VMEM((heads, size, width), BF16),
            pltpu.VMEM((heads, size, width), BF16),
            pltpu.VMEM((8, length), F32),
            pltpu.VMEM((length, width), F32),
            pltpu.VMEM((group - 1, length, width), F32),
            dma((4,)),
            dma((6,)),
            dma((heads,)),
            pltpu.SemaphoreType.REGULAR,
            dma((stages, parts, heads)),
            dma((parts, heads)),
            dma((stages, group - 1, parts, heads)),
            dma((stages, group - 1, parts, heads)),
            dma((stages, parts, heads)),
            dma((parts, heads)),
            dma((group - 1,)),
            dma((group - 1,)),
        ],
        compiler_params=pltpu.CompilerParams(
            collective_id=0, has_side_effects=True, vmem_limit_bytes=60 * 1024 * 1024
        ),
    )(
        tokens[0],
        query_matrix[0],
        key_matrix[0],
        value_matrix[0],
        output_gate_weight[0],
        rows_of(strength_weight),
        rows_of(decay_input_weight),
        decay_scale_table,
        log_spike_decay[0].T,
        head_norm_gain,
        closing_norm_gain[None],
    )
    return result[None]


def solution(mesh):
    placed = (
        P("pp", "fs", "tp"),
        P("pp", None, "tp"),
        P("pp", None, "tp"),
        P("pp", None, "tp"),
        P("pp", None, "tp"),
        P("pp", None, "tp"),
        P("pp", None, "tp"),
        P("pp", "tp"),
        P("pp", None, "tp"),
        P("pp", "tp"),
        P("tp"),
    )
    return jax.shard_map(
        functools.partial(on_device, mesh.shape["pp"], mesh.shape["tp"]),
        mesh=mesh,
        in_specs=placed,
        out_specs=P("pp", "fs", "tp"),
        check_vma=False,
    )
```

```python
import functools
import jax
import jax.numpy as jnp
from jax import lax
from jax.experimental import pallas as pl
from jax.experimental.pallas import tpu as pltpu
from jax.sharding import PartitionSpec as P

epsilon = 1e-06
F32 = jnp.float32
BF16 = jnp.bfloat16
MESH = pl.DeviceIdType.MESH
NT = (((1,), (1,)), ((), ()))


def silu(a):
    return a * (0.5 + 0.5 * jnp.tanh(0.5 * a))


def dot(a, b):
    return jnp.dot(a.astype(BF16), b.astype(BF16), preferred_element_type=F32)


def stack_kernel(
    stages,
    group,
    size,
    tokens,
    query_hbm,
    key_hbm,
    value_hbm,
    gate_hbm,
    strength_hbm,
    decay_in_hbm,
    decay_speed_hbm,
    spike_hbm,
    gain_hbm,
    closing_hbm,
    out,
    strength,
    decay_in,
    decay_speed,
    spike,
    gain,
    closing_gain,
    weights,
    acc,
    squares_own,
    beta_own,
    decay_own,
    decay_wide,
    speed_wide,
    spike_wide,
    xin,
    xout,
    yin,
    past_key,
    past_value,
    past_fade,
    part_mine,
    part_other,
    w_sem,
    small_sem,
    token_sem,
    go_sem,
    in_sem,
    entry_sem,
    fwd_send,
    fwd_recv,
    out_send,
    y_recv,
    part_send,
    part_recv,
):
    stage = lax.axis_index("pp")
    core = lax.axis_index("tp")
    last = stages - 1
    length, half = tokens.shape
    heads = xout.shape[1]
    width = half // heads
    model_width = group * half
    others = range(1, group)
    spans = [slice(start, start + size) for start in range(0, length, size)]

    def peer(d):
        return lax.rem(core + d, group)

    barrier = pltpu.get_barrier_semaphore()

    @pl.when(stage > 0)
    def _():
        pl.semaphore_signal(barrier, inc=1, device_id={"pp": stage - 1}, device_id_type=MESH)

    @pl.when(stage < last)
    def _():
        pl.semaphore_signal(barrier, inc=1, device_id={"pp": stage + 1}, device_id_type=MESH)

    for d in others:
        pl.semaphore_signal(barrier, inc=1, device_id={"tp": peer(d)}, device_id_type=MESH)

    def token_copy(h, target):
        return pltpu.make_async_copy(
            tokens.at[:, h * width : (h + 1) * width], target, token_sem.at[h]
        )

    @pl.when(stage == 0)
    def _():
        for h in range(heads):
            token_copy(h, xin.at[0, core * heads + h]).start()

    @pl.when(stage > 0)
    def _():
        for h in range(heads):
            token_copy(h, xout.at[stages, h]).start()

    small_loads = [
        pltpu.make_async_copy(a, b, small_sem.at[i])
        for i, (a, b) in enumerate(
            (
                (strength_hbm, strength),
                (decay_in_hbm, decay_in),
                (decay_speed_hbm, decay_speed),
                (spike_hbm, spike),
                (gain_hbm, gain),
                (closing_hbm, closing_gain),
            )
        )
    ]
    for load in small_loads:
        load.start()
    loads = [
        pltpu.make_async_copy(ref, weights.at[i], w_sem.at[i])
        for i, ref in enumerate((key_hbm, query_hbm, value_hbm, gate_hbm))
    ]
    for load in loads:
        load.start()

    def entry_copy(h, span):
        return pltpu.make_async_remote_copy(
            src_ref=xout.at[stages, h, span],
            dst_ref=xin.at[stage, core * heads + h, span],
            send_sem=entry_sem.at[span.start // size, h],
            recv_sem=in_sem.at[stage, span.start // size, h],
            device_id={"pp": 0},
            device_id_type=MESH,
        )

    def next_copy(m, h, span):
        return pltpu.make_async_remote_copy(
            src_ref=xout.at[m, h, span],
            dst_ref=xin.at[m, core * heads + h, span],
            send_sem=out_send.at[m, span.start // size, h],
            recv_sem=in_sem.at[m, span.start // size, h],
            device_id={"pp": lax.rem(stage + 1, stages)},
            device_id_type=MESH,
        )

    def exit_copy(m, h, span):
        return pltpu.make_async_remote_copy(
            src_ref=xout.at[m, h, span],
            dst_ref=yin.at[h, span],
            send_sem=out_send.at[m, span.start // size, h],
            recv_sem=y_recv.at[span.start // size, h],
            device_id={"pp": m},
            device_id_type=MESH,
        )

    def forward_copy(m, d, h, span):
        return pltpu.make_async_remote_copy(
            src_ref=xin.at[m, core * heads + h, span],
            dst_ref=xin.at[m, core * heads + h, span],
            send_sem=fwd_send.at[m, d - 1, span.start // size, h],
            recv_sem=fwd_recv.at[m, d - 1, span.start // size, h],
            device_id={"tp": peer(d)},
            device_id_type=MESH,
        )

    for h in range(heads):
        token_copy(h, xout.at[stages, h]).wait()
    pl.semaphore_wait(
        barrier, group - 1 + (stage > 0).astype(jnp.int32) + (stage < last).astype(jnp.int32)
    )

    @pl.when(stage == 0)
    def _():
        for span in spans:
            for h in range(heads):
                for d in others:
                    forward_copy(0, d, h, span).start()

    @pl.when(stage == 1)
    def _():
        for span in spans:
            for h in range(heads):
                entry_copy(h, span).start()

    for load in small_loads:
        load.wait()
    side = min(length // size, heads)
    groups = heads // side
    lanes = side * size
    block = min(16, size)
    pieces = size // block
    every = range(groups)
    spike_columns = jnp.concatenate(
        [spike[...], jnp.zeros((length - heads, length), F32)], axis=0
    ).T
    for g in every:
        for p in range(side):
            h = g + p * groups
            at = slice(g * lanes + p * size, g * lanes + (p + 1) * size)
            speed_wide[:, at] = jnp.broadcast_to(decay_speed[:, h : h + 1], (1, size))
        spread = jnp.broadcast_to(spike_columns[:, g : g + 1], (length, lanes))
        for p in range(1, side):
            h = g + p * groups
            lane = lax.broadcasted_iota(jnp.int32, (length, lanes), 1)
            other = jnp.broadcast_to(spike_columns[:, h : h + 1], (length, lanes))
            spread = jnp.where(lane >= p * size, other, spread)
        spike_wide[:, g * lanes : (g + 1) * lanes] = spread
    tile = min(256, model_width)
    same = lax.broadcasted_iota(jnp.int32, (tile, tile), 0) == lax.broadcasted_iota(
        jnp.int32, (tile, tile), 1
    )
    identity = jnp.where(same, 1.0, 0.0).astype(BF16)
    for start in range(0, model_width, tile):
        part = decay_in[:heads, start : start + tile].astype(F32)
        wide = jnp.concatenate(
            [
                jnp.broadcast_to(part[g + p * groups : g + p * groups + 1], (size, tile))
                for g in every
                for p in range(side)
            ],
            axis=0,
        ).astype(BF16)
        decay_wide[start : start + tile, :] = lax.dot_general(
            identity, wide, NT, preferred_element_type=F32
        ).astype(BF16)

    def gather(m, which, span):
        return jnp.concatenate([xin[m, which * heads + h, span] for h in range(heads)], axis=1)

    def glance(x, which):
        own = pl.ds(pl.multiple_of(which * half, half), half)
        wide = x.astype(F32)
        squares = jnp.sum(wide * wide, axis=1, keepdims=True)
        decay = dot(x, decay_wide[own, :])
        beta = lax.dot_general(x, strength[:, own], NT, preferred_element_type=F32)
        return squares, decay, beta[:, :heads]

    def project(x, which):
        own = pl.ds(pl.multiple_of(which * half, half), half)
        return [dot(x, weights[i, own, :]) for i in range(4)]

    def begin(m, span):
        own = pl.ds(pl.multiple_of(core * half, half), half)

        def first():
            x = gather(m, core, span)
            squares, decay, beta = glance(x, core)
            squares_own[span] = jnp.broadcast_to(squares, (size, width))
            decay_own[span] = decay
            beta_own[span] = beta

        def piece(i):
            acc[i, span] = dot(gather(m, core, span), weights[i, own, :])

        return [first] + [functools.partial(piece, i) for i in range(4)]

    def chunk(m, span, keep, use, between):
        squares = squares_own[span, :1]
        decay = decay_own[span]
        beta = beta_own[span]
        for d in others:
            for h in range(heads):
                forward_copy(m, d, h, span).wait_recv()
            source = peer(group - d)
            x = gather(m, source, span)
            squares_other, decay_other, beta_other = glance(x, source)
            squares = squares + squares_other
            decay = decay + decay_other
            beta = beta + beta_other
            mats = project(x, source)
            if d < group - 1:
                for i in range(4):
                    acc[i, span] += mats[i]
        inv_rms = lax.rsqrt(squares / model_width + epsilon)

        row = lax.broadcasted_iota(jnp.int32, (size, lanes), 0)
        lane = lax.broadcasted_iota(jnp.int32, (size, lanes), 1)
        column = lane % size
        band = (lax.broadcasted_iota(jnp.int32, (8, lanes), 1) % size) // block

        beta = 1.0 / (1.0 + jnp.exp(-beta * inv_rms))
        pre = decay * inv_rms
        softplus = jnp.maximum(pre, 0.0) + jnp.log(1.0 + jnp.exp(-jnp.abs(pre)))
        log_decay = spike_wide[span, :] - speed_wide[...] * softplus
        lower = jnp.where(
            lax.broadcasted_iota(jnp.int32, (size, size), 0)
            >= lax.broadcasted_iota(jnp.int32, (size, size), 1),
            1.0,
            0.0,
        ).astype(BF16)
        high = log_decay.astype(BF16)
        rest = log_decay - high.astype(F32)
        after = jnp.concatenate([row > column] * groups, axis=1)

        def total(mask):
            picked = (jnp.where(after, a.astype(F32), 0.0) if mask else a for a in (high, rest))
            return sum(dot(lower, a) for a in picked)

        since = total(True)
        if use:
            whole = total(False)

        def packed(which, g):
            return jnp.concatenate([which[g + p * groups] for p in range(side)], axis=1)

        def apart(which, g):
            empty = jnp.zeros_like(which[0])
            return jnp.concatenate(
                [
                    jnp.concatenate(
                        [which[g + p * groups] if s == p else empty for s in range(side)], axis=1
                    )
                    for p in range(side)
                ],
                axis=0,
            )

        def stacked(square):
            if side == 1:
                return square
            return jnp.concatenate(
                [jnp.where(lane // size == p, square, jnp.zeros_like(square)) for p in range(side)],
                axis=0,
            )

        def columns(i, h):
            part = slice(h * width, (h + 1) * width)
            return (acc[i, span, part] + mats[i][:, part]) * inv_rms

        def norm(a):
            return lax.rsqrt(jnp.sum(a * a, axis=1, keepdims=True) + epsilon)

        keys = [silu(columns(0, h)) for h in range(heads)]
        rounded_keys = [a.astype(BF16) for a in keys]
        queries = [silu(columns(1, h)) for h in range(heads)]
        rounded_queries = [a.astype(BF16) for a in queries]
        gram = []
        for g in every:
            left = jnp.concatenate([packed(rounded_keys, g), packed(rounded_queries, g)], axis=0)
            gram.append(
                lax.dot_general(left, apart(rounded_keys, g), NT, preferred_element_type=F32)
            )
        key_scale = [norm(a) for a in keys]
        query_scale = [norm(a) * width ** (-0.5) for a in queries]
        force = [beta[:, h : h + 1] * key_scale[h] for h in range(heads)]
        weight = [force[h] * key_scale[h] for h in range(heads)]
        values = [silu(columns(2, h)) * force[h] for h in range(heads)]

        def stretch(parts, g):
            out = jnp.broadcast_to(parts[g], (size, lanes))
            for p in range(1, side):
                out = jnp.where(
                    lane >= p * size, jnp.broadcast_to(parts[g + p * groups], (size, lanes)), out
                )
            return out

        def section(wide, g):
            return wide[:, g * lanes : (g + 1) * lanes]

        decayed = [jnp.where(row >= column, jnp.exp(section(since, g)), 0.0) for g in every]
        scale = [stretch(weight, g) for g in every]
        system = [
            jnp.where(row > column, gram[g][:size] * decayed[g], 0.0) * scale[g] for g in every
        ]
        scores = [(gram[g][size:] * decayed[g]).astype(BF16) for g in every]

        before = None
        if use:
            past_keys = [past_key[h] for h in range(heads)]
            past_values = [past_value[h] for h in range(heads)]
            before = []
            for g in every:
                left = jnp.concatenate(
                    [packed(rounded_keys, g), packed(rounded_queries, g)], axis=0
                )
                cross = lax.dot_general(left, apart(past_keys, g), NT, preferred_element_type=F32)
                fade = jnp.exp(section(whole, g) + past_fade[g : g + 1, :])
                cross = (cross * jnp.concatenate([fade, fade], axis=0)).astype(BF16)
                before.append(
                    jnp.dot(cross, apart(past_values, g), preferred_element_type=F32)
                )
            for g in every:
                for p in range(side):
                    h = g + p * groups
                    part = slice(p * width, (p + 1) * width)
                    values[h] = values[h] - weight[h] * before[g][:size, part]

        tiles = block // 8
        inverse = []
        for g in every:
            compact = []
            for t in range(tiles):
                tile = system[g][t * 8 : t * 8 + 8]
                for r in range(1, pieces):
                    at = r * block + t * 8
                    tile = jnp.where(band == r, system[g][at : at + 8], tile)
                compact.append(tile)
            inner = lax.broadcasted_iota(jnp.int32, (8, lanes), 1) % block
            down_rows = lax.broadcasted_iota(jnp.int32, (8, lanes), 0)
            solved = [
                jnp.where(down_rows + t * 8 == inner, 1.0, 0.0).astype(F32) for t in range(tiles)
            ]
            start_of = lax.broadcasted_iota(jnp.int32, (8, lanes), 1) - inner
            for j in range(block - 1):
                source = jnp.broadcast_to(
                    solved[j // 8][j % 8 : j % 8 + 1, :], (8, lanes)
                )
                for t in range((j + 1) // 8, tiles):
                    factor = jnp.take_along_axis(
                        compact[t], start_of + j, axis=1, mode="promise_in_bounds"
                    )
                    solved[t] = solved[t] - factor * source
            inverse.append(
                jnp.concatenate(
                    [
                        jnp.where(band == r, solved[t], 0.0).astype(F32)
                        for r in range(pieces)
                        for t in range(tiles)
                    ],
                    axis=0,
                ).astype(BF16)
            )
        queue = between()

        def fill(count):
            for _ in range(min(count, len(queue))):
                queue.pop(0)()

        update = [dot(inverse[g], apart([a.astype(BF16) for a in values], g)) for g in every]

        def split(wide):
            return [
                wide[h % groups][:, (h // groups) * width : (h // groups + 1) * width].astype(BF16)
                for h in range(heads)
            ]

        if pieces > 1:
            outside = row // block != column // block
            chain = [
                dot(inverse[g], stacked(jnp.where(outside, system[g], 0.0).astype(BF16)))
                for g in every
            ]
            fill(2)
            sign = -1.0
            done = 1
            while done < pieces:
                rounded = [chain[g].astype(BF16) for g in every]
                current = split(update)
                update = [
                    update[g] + sign * dot(rounded[g], apart(current, g)) for g in every
                ]
                done *= 2
                sign = 1.0
                if done < pieces:
                    chain = [dot(rounded[g], stacked(rounded[g])) for g in every]
                fill(1)
        final = split(update)
        mixed = [dot(scores[g], apart(final, g)) for g in every]
        fill(len(queue))
        if use:
            mixed = [mixed[g] + before[g][size:] for g in every]
        for h in range(heads):
            part = slice((h // groups) * width, (h // groups + 1) * width)
            raw = mixed[h % groups][:, part]
            gate = silu(columns(3, h)) * gain[:, h * width : (h + 1) * width]
            mean = jnp.mean(raw * raw, axis=1, keepdims=True)
            unit = query_scale[h]
            head_out = raw * (unit * lax.rsqrt(unit * unit * mean + epsilon)) * gate
            x = xin[m, core * heads + h, span].astype(F32)
            xout[m, h, span] = (x + head_out.astype(BF16).astype(F32)).astype(BF16)
        if keep:
            for h in range(heads):
                past_key[h] = rounded_keys[h]
                past_value[h] = final[h]
            for g in every:
                past_fade[g : g + 1, :] = section(since, g)[size - 1 : size, :]

    def arrive(m, span):
        for h in range(heads):
            next_copy(m, h, span).wait_recv()
            for d in others:
                forward_copy(m, d, h, span).start()

    def leave(m, span):
        @pl.when(stage < last)
        def _():
            for h in range(heads):
                next_copy(m, h, span).start()

        @pl.when((stage == last) & (m < last))
        def _():
            for h in range(heads):
                exit_copy(m, h, span).start()

    def step(m, _):
        for i, span in enumerate(spans):

            def between(i=i):
                if i + 1 < len(spans):
                    following, ahead = m, spans[i + 1]

                    @pl.when((stage > 0) | (m > 0))
                    def _():
                        arrive(following, ahead)

                else:
                    following, ahead = lax.rem(m + 1, stages), spans[0]

                    @pl.when(m < last)
                    def _():
                        arrive(following, ahead)

                return begin(following, ahead)

            chunk(m, span, keep=i + 1 < len(spans), use=i > 0, between=between)
            leave(m, span)
        return 0

    @pl.when(stage > 1)
    def _():
        pl.semaphore_wait(go_sem, 1)
        for span in spans:
            for h in range(heads):
                entry_copy(h, span).start()

    @pl.when(stage > 0)
    def _():
        entry_copy(heads - 1, spans[0]).wait_send()

    @pl.when((stage > 0) & (stage < last))
    def _():
        pl.semaphore_signal(go_sem, inc=1, device_id={"pp": stage + 1}, device_id_type=MESH)

    @pl.when(stage > 0)
    def _():
        arrive(0, spans[0])

    for i, piece in enumerate(begin(0, spans[0])):
        if i > 0:
            loads[i - 1].wait()
        piece()

    lax.fori_loop(0, stages, step, 0)

    @pl.when(stage == last)
    def _():
        for h in range(heads):
            yin[h] = xout[last, h]

    @pl.when(stage < last)
    def _():
        for span in spans:
            for h in range(heads):
                exit_copy(0, h, span).wait_recv()

    final = [yin[h].astype(F32) for h in range(heads)]
    total = sum(jnp.sum(a * a, axis=1, keepdims=True) for a in final)
    part_mine[...] = jnp.broadcast_to(total, part_mine.shape)
    part_copies = [
        pltpu.make_async_remote_copy(
            src_ref=part_mine,
            dst_ref=part_other.at[d - 1],
            send_sem=part_send.at[d - 1],
            recv_sem=part_recv.at[d - 1],
            device_id={"tp": peer(d)},
            device_id_type=MESH,
        )
        for d in others
    ]
    for copy in part_copies:
        copy.start()

    @pl.when(stage > 0)
    def _():
        for span in spans:
            for h in range(heads):
                if h < heads - 1 or span is not spans[0]:
                    entry_copy(h, span).wait_send()

    def drain(m, _):
        for span in spans:
            for h in range(heads):
                for d in others:
                    forward_copy(m, d, h, span).wait_send()

        @pl.when((stage < last) | (m < last))
        def _():
            for span in spans:
                for h in range(heads):
                    next_copy(m, h, span).wait_send()

        return 0

    lax.fori_loop(0, stages, drain, 0)
    total = part_mine[...]
    for copy in part_copies:
        copy.wait()
    for d in others:
        total = total + part_other[d - 1]
    inv_rms = lax.rsqrt(total / model_width + epsilon)
    for h in range(heads):
        part = slice(h * width, (h + 1) * width)
        out[:, part] = (final[h] * inv_rms * closing_gain[:, part]).astype(BF16)


def on_device(
    stages,
    group,
    tokens,
    query_matrix,
    key_matrix,
    value_matrix,
    output_gate_weight,
    strength_weight,
    decay_input_weight,
    decay_scale_table,
    log_spike_decay,
    head_norm_gain,
    closing_norm_gain,
):
    _, length, half = tokens.shape
    heads = strength_weight.shape[-1]
    width = half // heads
    parts = 2 if heads % 2 == 0 else 1
    size = length // parts

    def rows_of(weight):
        return jnp.pad(weight[0].T, ((0, 1), (0, 0))) if heads == 1 else weight[0].T

    vmem = pl.BlockSpec(memory_space=pltpu.VMEM)
    anywhere = pl.BlockSpec(memory_space=pltpu.HBM)
    dma = pltpu.SemaphoreType.DMA
    result = pl.pallas_call(
        functools.partial(stack_kernel, stages, group, size),
        out_shape=pltpu.VMEM((length, half), BF16),
        in_specs=[anywhere] * 11,
        out_specs=vmem,
        scratch_shapes=[
            pltpu.VMEM((max(heads, 2), group * half), BF16),
            pltpu.VMEM((max(heads, 2), group * half), BF16),
            pltpu.VMEM((1, heads), F32),
            pltpu.VMEM((heads, length), F32),
            pltpu.VMEM((1, half), F32),
            pltpu.VMEM((1, half), F32),
            pltpu.VMEM((4, group * half, half), BF16),
            pltpu.VMEM((4, length, half), F32),
            pltpu.VMEM((length, width), F32),
            pltpu.VMEM((length, heads), F32),
            pltpu.VMEM((length, heads * size), F32),
            pltpu.VMEM((group * half, heads * size), BF16),
            pltpu.VMEM((1, heads * size), F32),
            pltpu.VMEM((length, heads * size), F32),
            pltpu.VMEM((stages, group * heads, length, width), BF16),
            pltpu.VMEM((stages + 1, heads, length, width), BF16),
            pltpu.VMEM((heads, length, width), BF16),
            pltpu.VMEM((heads, size, width), BF16),
            pltpu.VMEM((heads, size, width), BF16),
            pltpu.VMEM((8, length), F32),
            pltpu.VMEM((length, width), F32),
            pltpu.VMEM((group - 1, length, width), F32),
            dma((4,)),
            dma((6,)),
            dma((heads,)),
            pltpu.SemaphoreType.REGULAR,
            dma((stages, parts, heads)),
            dma((parts, heads)),
            dma((stages, group - 1, parts, heads)),
            dma((stages, group - 1, parts, heads)),
            dma((stages, parts, heads)),
            dma((parts, heads)),
            dma((group - 1,)),
            dma((group - 1,)),
        ],
        compiler_params=pltpu.CompilerParams(
            collective_id=0, has_side_effects=True, vmem_limit_bytes=60 * 1024 * 1024
        ),
    )(
        tokens[0],
        query_matrix[0],
        key_matrix[0],
        value_matrix[0],
        output_gate_weight[0],
        rows_of(strength_weight),
        rows_of(decay_input_weight),
        decay_scale_table,
        log_spike_decay[0].T,
        head_norm_gain,
        closing_norm_gain[None],
    )
    return result[None]


def solution(mesh):
    placed = (
        P("pp", "fs", "tp"),
        P("pp", None, "tp"),
        P("pp", None, "tp"),
        P("pp", None, "tp"),
        P("pp", None, "tp"),
        P("pp", None, "tp"),
        P("pp", None, "tp"),
        P("pp", "tp"),
        P("pp", None, "tp"),
        P("pp", "tp"),
        P("tp"),
    )
    return jax.shard_map(
        functools.partial(on_device, mesh.shape["pp"], mesh.shape["tp"]),
        mesh=mesh,
        in_specs=placed,
        out_specs=P("pp", "fs", "tp"),
        check_vma=False,
    )
```

```python
import functools
import jax
import jax.numpy as jnp
from jax import lax
from jax.experimental import pallas as pl
from jax.experimental.pallas import tpu as pltpu
from jax.sharding import PartitionSpec as P

epsilon = 1e-06
F32 = jnp.float32
BF16 = jnp.bfloat16
MESH = pl.DeviceIdType.MESH
NT = (((1,), (1,)), ((), ()))


def silu(a):
    return a * (0.5 + 0.5 * jnp.tanh(0.5 * a))


def dot(a, b):
    return jnp.dot(a.astype(BF16), b.astype(BF16), preferred_element_type=F32)


def stack_kernel(
    stages,
    group,
    size,
    tokens,
    query_hbm,
    key_hbm,
    value_hbm,
    gate_hbm,
    strength_hbm,
    decay_in_hbm,
    decay_speed_hbm,
    spike_hbm,
    gain_hbm,
    closing_hbm,
    out,
    strength,
    decay_in,
    decay_speed,
    spike,
    gain,
    closing_gain,
    weights,
    acc,
    squares_own,
    beta_own,
    decay_own,
    decay_wide,
    speed_wide,
    spike_wide,
    xin,
    xout,
    yin,
    past_key,
    past_value,
    past_fade,
    part_mine,
    part_other,
    w_sem,
    small_sem,
    token_sem,
    go_sem,
    in_sem,
    entry_sem,
    fwd_send,
    fwd_recv,
    out_send,
    y_recv,
    part_send,
    part_recv,
):
    stage = lax.axis_index("pp")
    core = lax.axis_index("tp")
    last = stages - 1
    length, half = tokens.shape
    heads = xout.shape[1]
    width = half // heads
    model_width = group * half
    others = range(1, group)
    spans = [slice(start, start + size) for start in range(0, length, size)]

    def peer(d):
        return lax.rem(core + d, group)

    barrier = pltpu.get_barrier_semaphore()

    @pl.when(stage > 0)
    def _():
        pl.semaphore_signal(barrier, inc=1, device_id={"pp": stage - 1}, device_id_type=MESH)

    @pl.when(stage < last)
    def _():
        pl.semaphore_signal(barrier, inc=1, device_id={"pp": stage + 1}, device_id_type=MESH)

    for d in others:
        pl.semaphore_signal(barrier, inc=1, device_id={"tp": peer(d)}, device_id_type=MESH)

    def token_copy(h, target):
        return pltpu.make_async_copy(
            tokens.at[:, h * width : (h + 1) * width], target, token_sem.at[h]
        )

    @pl.when(stage == 0)
    def _():
        for h in range(heads):
            token_copy(h, xin.at[0, core * heads + h]).start()

    @pl.when(stage > 0)
    def _():
        for h in range(heads):
            token_copy(h, xout.at[stages, h]).start()

    small_loads = [
        pltpu.make_async_copy(a, b, small_sem.at[i])
        for i, (a, b) in enumerate(
            (
                (strength_hbm, strength),
                (decay_in_hbm, decay_in),
                (decay_speed_hbm, decay_speed),
                (spike_hbm, spike),
                (gain_hbm, gain),
                (closing_hbm, closing_gain),
            )
        )
    ]
    for load in small_loads:
        load.start()
    loads = [
        pltpu.make_async_copy(ref, weights.at[i], w_sem.at[i])
        for i, ref in enumerate((key_hbm, query_hbm, value_hbm, gate_hbm))
    ]
    for load in loads:
        load.start()

    def entry_copy(h, span):
        return pltpu.make_async_remote_copy(
            src_ref=xout.at[stages, h, span],
            dst_ref=xin.at[stage, core * heads + h, span],
            send_sem=entry_sem.at[span.start // size, h],
            recv_sem=in_sem.at[stage, span.start // size, h],
            device_id={"pp": 0},
            device_id_type=MESH,
        )

    def next_copy(m, h, span):
        return pltpu.make_async_remote_copy(
            src_ref=xout.at[m, h, span],
            dst_ref=xin.at[m, core * heads + h, span],
            send_sem=out_send.at[m, span.start // size, h],
            recv_sem=in_sem.at[m, span.start // size, h],
            device_id={"pp": lax.rem(stage + 1, stages)},
            device_id_type=MESH,
        )

    def exit_copy(m, h, span):
        return pltpu.make_async_remote_copy(
            src_ref=xout.at[m, h, span],
            dst_ref=yin.at[h, span],
            send_sem=out_send.at[m, span.start // size, h],
            recv_sem=y_recv.at[span.start // size, h],
            device_id={"pp": m},
            device_id_type=MESH,
        )

    def forward_copy(m, d, h, span):
        return pltpu.make_async_remote_copy(
            src_ref=xin.at[m, core * heads + h, span],
            dst_ref=xin.at[m, core * heads + h, span],
            send_sem=fwd_send.at[m, d - 1, span.start // size, h],
            recv_sem=fwd_recv.at[m, d - 1, span.start // size, h],
            device_id={"tp": peer(d)},
            device_id_type=MESH,
        )

    for h in range(heads):
        token_copy(h, xout.at[stages, h]).wait()
    pl.semaphore_wait(
        barrier, group - 1 + (stage > 0).astype(jnp.int32) + (stage < last).astype(jnp.int32)
    )

    @pl.when(stage == 0)
    def _():
        for span in spans:
            for h in range(heads):
                for d in others:
                    forward_copy(0, d, h, span).start()

    @pl.when(stage == 1)
    def _():
        for span in spans:
            for h in range(heads):
                entry_copy(h, span).start()

    for load in small_loads:
        load.wait()
    side = min(length // size, heads)
    groups = heads // side
    lanes = side * size
    block = min(16, size)
    pieces = size // block
    every = range(groups)
    spike_columns = jnp.concatenate(
        [spike[...], jnp.zeros((length - heads, length), F32)], axis=0
    ).T
    for g in every:
        for p in range(side):
            h = g + p * groups
            at = slice(g * lanes + p * size, g * lanes + (p + 1) * size)
            speed_wide[:, at] = jnp.broadcast_to(decay_speed[:, h : h + 1], (1, size))
        spread = jnp.broadcast_to(spike_columns[:, g : g + 1], (length, lanes))
        for p in range(1, side):
            h = g + p * groups
            lane = lax.broadcasted_iota(jnp.int32, (length, lanes), 1)
            other = jnp.broadcast_to(spike_columns[:, h : h + 1], (length, lanes))
            spread = jnp.where(lane >= p * size, other, spread)
        spike_wide[:, g * lanes : (g + 1) * lanes] = spread
    tile = min(256, model_width)
    same = lax.broadcasted_iota(jnp.int32, (tile, tile), 0) == lax.broadcasted_iota(
        jnp.int32, (tile, tile), 1
    )
    identity = jnp.where(same, 1.0, 0.0).astype(BF16)
    for start in range(0, model_width, tile):
        part = decay_in[:heads, start : start + tile].astype(F32)
        wide = jnp.concatenate(
            [
                jnp.broadcast_to(part[g + p * groups : g + p * groups + 1], (size, tile))
                for g in every
                for p in range(side)
            ],
            axis=0,
        ).astype(BF16)
        decay_wide[start : start + tile, :] = lax.dot_general(
            identity, wide, NT, preferred_element_type=F32
        ).astype(BF16)

    def gather(m, which, span):
        return jnp.concatenate([xin[m, which * heads + h, span] for h in range(heads)], axis=1)

    def glance(x, which):
        own = pl.ds(pl.multiple_of(which * half, half), half)
        wide = x.astype(F32)
        squares = jnp.sum(wide * wide, axis=1, keepdims=True)
        decay = dot(x, decay_wide[own, :])
        beta = lax.dot_general(x, strength[:, own], NT, preferred_element_type=F32)
        return squares, decay, beta[:, :heads]

    def project(x, which):
        own = pl.ds(pl.multiple_of(which * half, half), half)
        return [dot(x, weights[i, own, :]) for i in range(4)]

    def begin(m, span):
        own = pl.ds(pl.multiple_of(core * half, half), half)

        def first():
            x = gather(m, core, span)
            squares, decay, beta = glance(x, core)
            squares_own[span] = jnp.broadcast_to(squares, (size, width))
            decay_own[span] = decay
            beta_own[span] = beta

        def piece(i):
            acc[i, span] = dot(gather(m, core, span), weights[i, own, :])

        return [first] + [functools.partial(piece, i) for i in range(4)]

    def chunk(m, span, keep, use, between):
        squares = squares_own[span, :1]
        decay = decay_own[span]
        beta = beta_own[span]
        for d in others:
            for h in range(heads):
                forward_copy(m, d, h, span).wait_recv()
            source = peer(group - d)
            x = gather(m, source, span)
            squares_other, decay_other, beta_other = glance(x, source)
            squares = squares + squares_other
            decay = decay + decay_other
            beta = beta + beta_other
            mats = project(x, source)
            if d < group - 1:
                for i in range(4):
                    acc[i, span] += mats[i]
        inv_rms = lax.rsqrt(squares / model_width + epsilon)

        row = lax.broadcasted_iota(jnp.int32, (size, lanes), 0)
        lane = lax.broadcasted_iota(jnp.int32, (size, lanes), 1)
        column = lane % size
        band = (lax.broadcasted_iota(jnp.int32, (8, lanes), 1) % size) // block

        beta = 1.0 / (1.0 + jnp.exp(-beta * inv_rms))
        pre = decay * inv_rms
        softplus = jnp.maximum(pre, 0.0) + jnp.log(1.0 + jnp.exp(-jnp.abs(pre)))
        log_decay = spike_wide[span, :] - speed_wide[...] * softplus
        lower = jnp.where(
            lax.broadcasted_iota(jnp.int32, (size, size), 0)
            >= lax.broadcasted_iota(jnp.int32, (size, size), 1),
            1.0,
            0.0,
        ).astype(BF16)
        high = log_decay.astype(BF16)
        rest = log_decay - high.astype(F32)
        after = jnp.concatenate([row > column] * groups, axis=1)

        def total(mask):
            picked = (jnp.where(after, a.astype(F32), 0.0) if mask else a for a in (high, rest))
            return sum(dot(lower, a) for a in picked)

        since = total(True)
        if use:
            whole = total(False)

        def packed(which, g):
            return jnp.concatenate([which[g + p * groups] for p in range(side)], axis=1)

        def apart(which, g):
            empty = jnp.zeros_like(which[0])
            return jnp.concatenate(
                [
                    jnp.concatenate(
                        [which[g + p * groups] if s == p else empty for s in range(side)], axis=1
                    )
                    for p in range(side)
                ],
                axis=0,
            )

        def stacked(square):
            if side == 1:
                return square
            return jnp.concatenate(
                [jnp.where(lane // size == p, square, jnp.zeros_like(square)) for p in range(side)],
                axis=0,
            )

        def columns(i, h):
            part = slice(h * width, (h + 1) * width)
            return (acc[i, span, part] + mats[i][:, part]) * inv_rms

        def norm(a):
            return lax.rsqrt(jnp.sum(a * a, axis=1, keepdims=True) + epsilon)

        keys = [silu(columns(0, h)) for h in range(heads)]
        rounded_keys = [a.astype(BF16) for a in keys]
        queries = [silu(columns(1, h)) for h in range(heads)]
        rounded_queries = [a.astype(BF16) for a in queries]
        gram = []
        for g in every:
            left = jnp.concatenate([packed(rounded_keys, g), packed(rounded_queries, g)], axis=0)
            gram.append(
                lax.dot_general(left, apart(rounded_keys, g), NT, preferred_element_type=F32)
            )
        key_scale = [norm(a) for a in keys]
        query_scale = [norm(a) * width ** (-0.5) for a in queries]
        force = [beta[:, h : h + 1] * key_scale[h] for h in range(heads)]
        weight = [force[h] * key_scale[h] for h in range(heads)]
        values = [silu(columns(2, h)) * force[h] for h in range(heads)]

        def stretch(parts, g):
            out = jnp.broadcast_to(parts[g], (size, lanes))
            for p in range(1, side):
                out = jnp.where(
                    lane >= p * size, jnp.broadcast_to(parts[g + p * groups], (size, lanes)), out
                )
            return out

        def section(wide, g):
            return wide[:, g * lanes : (g + 1) * lanes]

        decayed = [jnp.where(row >= column, jnp.exp(section(since, g)), 0.0) for g in every]
        scale = [stretch(weight, g) for g in every]
        system = [
            jnp.where(row > column, gram[g][:size] * decayed[g], 0.0) * scale[g] for g in every
        ]
        scores = [(gram[g][size:] * decayed[g]).astype(BF16) for g in every]

        before = None
        if use:
            past_keys = [past_key[h] for h in range(heads)]
            past_values = [past_value[h] for h in range(heads)]
            before = []
            for g in every:
                left = jnp.concatenate(
                    [packed(rounded_keys, g), packed(rounded_queries, g)], axis=0
                )
                cross = lax.dot_general(left, apart(past_keys, g), NT, preferred_element_type=F32)
                fade = jnp.exp(section(whole, g) + past_fade[g : g + 1, :])
                cross = (cross * jnp.concatenate([fade, fade], axis=0)).astype(BF16)
                before.append(
                    jnp.dot(cross, apart(past_values, g), preferred_element_type=F32)
                )
            for g in every:
                for p in range(side):
                    h = g + p * groups
                    part = slice(p * width, (p + 1) * width)
                    values[h] = values[h] - weight[h] * before[g][:size, part]

        tiles = block // 8
        inverse = []
        for g in every:
            compact = []
            for t in range(tiles):
                tile = system[g][t * 8 : t * 8 + 8]
                for r in range(1, pieces):
                    at = r * block + t * 8
                    tile = jnp.where(band == r, system[g][at : at + 8], tile)
                compact.append(tile)
            inner = lax.broadcasted_iota(jnp.int32, (8, lanes), 1) % block
            down_rows = lax.broadcasted_iota(jnp.int32, (8, lanes), 0)
            solved = [
                jnp.where(down_rows + t * 8 == inner, 1.0, 0.0).astype(F32) for t in range(tiles)
            ]
            start_of = lax.broadcasted_iota(jnp.int32, (8, lanes), 1) - inner
            for j in range(block - 1):
                source = jnp.broadcast_to(
                    solved[j // 8][j % 8 : j % 8 + 1, :], (8, lanes)
                )
                for t in range((j + 1) // 8, tiles):
                    factor = jnp.take_along_axis(
                        compact[t], start_of + j, axis=1, mode="promise_in_bounds"
                    )
                    solved[t] = solved[t] - factor * source
            inverse.append(
                jnp.concatenate(
                    [
                        jnp.where(band == r, solved[t], 0.0).astype(F32)
                        for r in range(pieces)
                        for t in range(tiles)
                    ],
                    axis=0,
                ).astype(BF16)
            )
        queue = between()

        def fill(count):
            for _ in range(min(count, len(queue))):
                queue.pop(0)()

        update = [dot(inverse[g], apart([a.astype(BF16) for a in values], g)) for g in every]

        def split(wide):
            return [
                wide[h % groups][:, (h // groups) * width : (h // groups + 1) * width].astype(BF16)
                for h in range(heads)
            ]

        if pieces > 1:
            outside = row // block != column // block
            chain = [
                dot(inverse[g], stacked(jnp.where(outside, system[g], 0.0).astype(BF16)))
                for g in every
            ]
            fill(2)
            sign = -1.0
            done = 1
            while done < pieces:
                rounded = [chain[g].astype(BF16) for g in every]
                current = split(update)
                update = [
                    update[g] + sign * dot(rounded[g], apart(current, g)) for g in every
                ]
                done *= 2
                sign = 1.0
                if done < pieces:
                    chain = [dot(rounded[g], stacked(rounded[g])) for g in every]
                fill(1)
        final = split(update)
        mixed = [dot(scores[g], apart(final, g)) for g in every]
        fill(len(queue))
        if use:
            mixed = [mixed[g] + before[g][size:] for g in every]
        for h in range(heads):
            part = slice((h // groups) * width, (h // groups + 1) * width)
            raw = mixed[h % groups][:, part]
            gate = silu(columns(3, h)) * gain[:, h * width : (h + 1) * width]
            mean = jnp.mean(raw * raw, axis=1, keepdims=True)
            unit = query_scale[h]
            head_out = raw * (unit * lax.rsqrt(unit * unit * mean + epsilon)) * gate
            x = xin[m, core * heads + h, span].astype(F32)
            xout[m, h, span] = (x + head_out.astype(BF16).astype(F32)).astype(BF16)
        if keep:
            for h in range(heads):
                past_key[h] = rounded_keys[h]
                past_value[h] = final[h]
            for g in every:
                past_fade[g : g + 1, :] = section(since, g)[size - 1 : size, :]

    def arrive(m, span):
        for h in range(heads):
            next_copy(m, h, span).wait_recv()
            for d in others:
                forward_copy(m, d, h, span).start()

    def leave(m, span):
        @pl.when(stage < last)
        def _():
            for h in range(heads):
                next_copy(m, h, span).start()

        @pl.when((stage == last) & (m < last))
        def _():
            for h in range(heads):
                exit_copy(m, h, span).start()

    def step(m, _):
        for i, span in enumerate(spans):

            def between(i=i):
                if i + 1 < len(spans):
                    following, ahead = m, spans[i + 1]

                    @pl.when((stage > 0) | (m > 0))
                    def _():
                        arrive(following, ahead)

                else:
                    following, ahead = lax.rem(m + 1, stages), spans[0]

                    @pl.when(m < last)
                    def _():
                        arrive(following, ahead)

                return begin(following, ahead)

            chunk(m, span, keep=i + 1 < len(spans), use=i > 0, between=between)
            leave(m, span)
        return 0

    @pl.when(stage > 1)
    def _():
        pl.semaphore_wait(go_sem, 1)
        for span in spans:
            for h in range(heads):
                entry_copy(h, span).start()

    @pl.when(stage == 1)
    def _():
        entry_copy(1, spans[0]).wait_send()

    @pl.when(stage > 1)
    def _():
        entry_copy(1, spans[-1]).wait_send()

    @pl.when((stage > 0) & (stage < last))
    def _():
        pl.semaphore_signal(go_sem, inc=1, device_id={"pp": stage + 1}, device_id_type=MESH)

    @pl.when(stage > 0)
    def _():
        arrive(0, spans[0])

    for load in loads:
        load.wait()
    for piece in begin(0, spans[0]):
        piece()

    lax.fori_loop(0, stages, step, 0)

    @pl.when(stage == last)
    def _():
        for h in range(heads):
            yin[h] = xout[last, h]

    @pl.when(stage < last)
    def _():
        for span in spans:
            for h in range(heads):
                exit_copy(0, h, span).wait_recv()

    final = [yin[h].astype(F32) for h in range(heads)]
    total = sum(jnp.sum(a * a, axis=1, keepdims=True) for a in final)
    part_mine[...] = jnp.broadcast_to(total, part_mine.shape)
    part_copies = [
        pltpu.make_async_remote_copy(
            src_ref=part_mine,
            dst_ref=part_other.at[d - 1],
            send_sem=part_send.at[d - 1],
            recv_sem=part_recv.at[d - 1],
            device_id={"tp": peer(d)},
            device_id_type=MESH,
        )
        for d in others
    ]
    for copy in part_copies:
        copy.start()

    @pl.when(stage > 0)
    def _():
        for span in spans:
            for h in range(heads):
                f1 = h == 1 and span is spans[0]
                f2 = h == 1 and span is spans[-1]
                wanted = (not f1) if f1 == f2 else (jnp.where(stage == 1, int(not f1), int(not f2)) == 1)

                @pl.when(wanted)
                def _(h=h, span=span):
                    entry_copy(h, span).wait_send()

    def drain(m, _):
        for span in spans:
            for h in range(heads):
                for d in others:
                    forward_copy(m, d, h, span).wait_send()

        @pl.when((stage < last) | (m < last))
        def _():
            for span in spans:
                for h in range(heads):
                    next_copy(m, h, span).wait_send()

        return 0

    lax.fori_loop(0, stages, drain, 0)
    total = part_mine[...]
    for copy in part_copies:
        copy.wait()
    for d in others:
        total = total + part_other[d - 1]
    inv_rms = lax.rsqrt(total / model_width + epsilon)
    for h in range(heads):
        part = slice(h * width, (h + 1) * width)
        out[:, part] = (final[h] * inv_rms * closing_gain[:, part]).astype(BF16)


def on_device(
    stages,
    group,
    tokens,
    query_matrix,
    key_matrix,
    value_matrix,
    output_gate_weight,
    strength_weight,
    decay_input_weight,
    decay_scale_table,
    log_spike_decay,
    head_norm_gain,
    closing_norm_gain,
):
    _, length, half = tokens.shape
    heads = strength_weight.shape[-1]
    width = half // heads
    parts = 2 if heads % 2 == 0 else 1
    size = length // parts

    def rows_of(weight):
        return jnp.pad(weight[0].T, ((0, 1), (0, 0))) if heads == 1 else weight[0].T

    vmem = pl.BlockSpec(memory_space=pltpu.VMEM)
    anywhere = pl.BlockSpec(memory_space=pltpu.HBM)
    dma = pltpu.SemaphoreType.DMA
    result = pl.pallas_call(
        functools.partial(stack_kernel, stages, group, size),
        out_shape=pltpu.VMEM((length, half), BF16),
        in_specs=[anywhere] * 11,
        out_specs=vmem,
        scratch_shapes=[
            pltpu.VMEM((max(heads, 2), group * half), BF16),
            pltpu.VMEM((max(heads, 2), group * half), BF16),
            pltpu.VMEM((1, heads), F32),
            pltpu.VMEM((heads, length), F32),
            pltpu.VMEM((1, half), F32),
            pltpu.VMEM((1, half), F32),
            pltpu.VMEM((4, group * half, half), BF16),
            pltpu.VMEM((4, length, half), F32),
            pltpu.VMEM((length, width), F32),
            pltpu.VMEM((length, heads), F32),
            pltpu.VMEM((length, heads * size), F32),
            pltpu.VMEM((group * half, heads * size), BF16),
            pltpu.VMEM((1, heads * size), F32),
            pltpu.VMEM((length, heads * size), F32),
            pltpu.VMEM((stages, group * heads, length, width), BF16),
            pltpu.VMEM((stages + 1, heads, length, width), BF16),
            pltpu.VMEM((heads, length, width), BF16),
            pltpu.VMEM((heads, size, width), BF16),
            pltpu.VMEM((heads, size, width), BF16),
            pltpu.VMEM((8, length), F32),
            pltpu.VMEM((length, width), F32),
            pltpu.VMEM((group - 1, length, width), F32),
            dma((4,)),
            dma((6,)),
            dma((heads,)),
            pltpu.SemaphoreType.REGULAR,
            dma((stages, parts, heads)),
            dma((parts, heads)),
            dma((stages, group - 1, parts, heads)),
            dma((stages, group - 1, parts, heads)),
            dma((stages, parts, heads)),
            dma((parts, heads)),
            dma((group - 1,)),
            dma((group - 1,)),
        ],
        compiler_params=pltpu.CompilerParams(
            collective_id=0, has_side_effects=True, vmem_limit_bytes=60 * 1024 * 1024
        ),
    )(
        tokens[0],
        query_matrix[0],
        key_matrix[0],
        value_matrix[0],
        output_gate_weight[0],
        rows_of(strength_weight),
        rows_of(decay_input_weight),
        decay_scale_table,
        log_spike_decay[0].T,
        head_norm_gain,
        closing_norm_gain[None],
    )
    return result[None]


def solution(mesh):
    placed = (
        P("pp", "fs", "tp"),
        P("pp", None, "tp"),
        P("pp", None, "tp"),
        P("pp", None, "tp"),
        P("pp", None, "tp"),
        P("pp", None, "tp"),
        P("pp", None, "tp"),
        P("pp", "tp"),
        P("pp", None, "tp"),
        P("pp", "tp"),
        P("tp"),
    )
    return jax.shard_map(
        functools.partial(on_device, mesh.shape["pp"], mesh.shape["tp"]),
        mesh=mesh,
        in_specs=placed,
        out_specs=P("pp", "fs", "tp"),
        check_vma=False,
    )
```

```python
import functools
import jax
import jax.numpy as jnp
from jax import lax
from jax.experimental import pallas as pl
from jax.experimental.pallas import tpu as pltpu
from jax.sharding import PartitionSpec as P

epsilon = 1e-06
F32 = jnp.float32
BF16 = jnp.bfloat16
MESH = pl.DeviceIdType.MESH
NT = (((1,), (1,)), ((), ()))


def silu(a):
    return a * (0.5 + 0.5 * jnp.tanh(0.5 * a))


def dot(a, b):
    return jnp.dot(a.astype(BF16), b.astype(BF16), preferred_element_type=F32)


def stack_kernel(
    stages,
    group,
    size,
    tokens,
    query_hbm,
    key_hbm,
    value_hbm,
    gate_hbm,
    strength_hbm,
    decay_in_hbm,
    decay_speed_hbm,
    spike_hbm,
    gain_hbm,
    closing_hbm,
    out,
    strength,
    decay_in,
    decay_speed,
    spike,
    gain,
    closing_gain,
    weights,
    acc,
    squares_own,
    beta_own,
    decay_own,
    decay_wide,
    speed_wide,
    spike_wide,
    xin,
    xout,
    yin,
    past_key,
    past_value,
    past_fade,
    part_mine,
    part_other,
    w_sem,
    small_sem,
    token_sem,
    go_sem,
    in_sem,
    entry_sem,
    fwd_send,
    fwd_recv,
    out_send,
    y_recv,
    part_send,
    part_recv,
):
    stage = lax.axis_index("pp")
    core = lax.axis_index("tp")
    last = stages - 1
    length, half = tokens.shape
    heads = xout.shape[1]
    width = half // heads
    model_width = group * half
    others = range(1, group)
    spans = [slice(start, start + size) for start in range(0, length, size)]

    def peer(d):
        return lax.rem(core + d, group)

    barrier = pltpu.get_barrier_semaphore()

    @pl.when(stage > 0)
    def _():
        pl.semaphore_signal(barrier, inc=1, device_id={"pp": stage - 1}, device_id_type=MESH)

    @pl.when(stage < last)
    def _():
        pl.semaphore_signal(barrier, inc=1, device_id={"pp": stage + 1}, device_id_type=MESH)

    for d in others:
        pl.semaphore_signal(barrier, inc=1, device_id={"tp": peer(d)}, device_id_type=MESH)

    def token_copy(h, target):
        return pltpu.make_async_copy(
            tokens.at[:, h * width : (h + 1) * width], target, token_sem.at[h]
        )

    @pl.when(stage == 0)
    def _():
        for h in range(heads):
            token_copy(h, xin.at[0, core * heads + h]).start()

    @pl.when(stage > 0)
    def _():
        for h in range(heads):
            token_copy(h, xout.at[stages, h]).start()

    small_loads = [
        pltpu.make_async_copy(a, b, small_sem.at[i])
        for i, (a, b) in enumerate(
            (
                (strength_hbm, strength),
                (decay_in_hbm, decay_in),
                (decay_speed_hbm, decay_speed),
                (spike_hbm, spike),
                (gain_hbm, gain),
                (closing_hbm, closing_gain),
            )
        )
    ]
    for load in small_loads:
        load.start()
    loads = [
        pltpu.make_async_copy(ref, weights.at[i], w_sem.at[i])
        for i, ref in enumerate((key_hbm, query_hbm, value_hbm, gate_hbm))
    ]
    for load in loads:
        load.start()

    def entry_copy(h, span):
        return pltpu.make_async_remote_copy(
            src_ref=xout.at[stages, h, span],
            dst_ref=xin.at[stage, core * heads + h, span],
            send_sem=entry_sem.at[span.start // size, h],
            recv_sem=in_sem.at[stage, span.start // size, h],
            device_id={"pp": 0},
            device_id_type=MESH,
        )

    def next_copy(m, h, span):
        return pltpu.make_async_remote_copy(
            src_ref=xout.at[m, h, span],
            dst_ref=xin.at[m, core * heads + h, span],
            send_sem=out_send.at[m, span.start // size, h],
            recv_sem=in_sem.at[m, span.start // size, h],
            device_id={"pp": lax.rem(stage + 1, stages)},
            device_id_type=MESH,
        )

    def exit_copy(m, h, span):
        return pltpu.make_async_remote_copy(
            src_ref=xout.at[m, h, span],
            dst_ref=yin.at[h, span],
            send_sem=out_send.at[m, span.start // size, h],
            recv_sem=y_recv.at[span.start // size, h],
            device_id={"pp": m},
            device_id_type=MESH,
        )

    def forward_copy(m, d, h, span):
        return pltpu.make_async_remote_copy(
            src_ref=xin.at[m, core * heads + h, span],
            dst_ref=xin.at[m, core * heads + h, span],
            send_sem=fwd_send.at[m, d - 1, span.start // size, h],
            recv_sem=fwd_recv.at[m, d - 1, span.start // size, h],
            device_id={"tp": peer(d)},
            device_id_type=MESH,
        )

    for h in range(heads):
        token_copy(h, xout.at[stages, h]).wait()
    pl.semaphore_wait(
        barrier, group - 1 + (stage > 0).astype(jnp.int32) + (stage < last).astype(jnp.int32)
    )

    @pl.when(stage == 0)
    def _():
        for span in spans:
            for h in range(heads):
                for d in others:
                    forward_copy(0, d, h, span).start()

    @pl.when(stage == 1)
    def _():
        for span in spans:
            for h in range(heads):
                entry_copy(h, span).start()

    for load in small_loads:
        load.wait()
    side = min(length // size, heads)
    groups = heads // side
    lanes = side * size
    block = min(16, size)
    pieces = size // block
    every = range(groups)
    spike_columns = jnp.concatenate(
        [spike[...], jnp.zeros((length - heads, length), F32)], axis=0
    ).T
    for g in every:
        for p in range(side):
            h = g + p * groups
            at = slice(g * lanes + p * size, g * lanes + (p + 1) * size)
            speed_wide[:, at] = jnp.broadcast_to(decay_speed[:, h : h + 1], (1, size))
        spread = jnp.broadcast_to(spike_columns[:, g : g + 1], (length, lanes))
        for p in range(1, side):
            h = g + p * groups
            lane = lax.broadcasted_iota(jnp.int32, (length, lanes), 1)
            other = jnp.broadcast_to(spike_columns[:, h : h + 1], (length, lanes))
            spread = jnp.where(lane >= p * size, other, spread)
        spike_wide[:, g * lanes : (g + 1) * lanes] = spread
    tile = min(256, model_width)
    same = lax.broadcasted_iota(jnp.int32, (tile, tile), 0) == lax.broadcasted_iota(
        jnp.int32, (tile, tile), 1
    )
    identity = jnp.where(same, 1.0, 0.0).astype(BF16)
    for start in range(0, model_width, tile):
        part = decay_in[:heads, start : start + tile].astype(F32)
        wide = jnp.concatenate(
            [
                jnp.broadcast_to(part[g + p * groups : g + p * groups + 1], (size, tile))
                for g in every
                for p in range(side)
            ],
            axis=0,
        ).astype(BF16)
        decay_wide[start : start + tile, :] = lax.dot_general(
            identity, wide, NT, preferred_element_type=F32
        ).astype(BF16)

    def gather(m, which, span):
        return jnp.concatenate([xin[m, which * heads + h, span] for h in range(heads)], axis=1)

    def glance(x, which):
        own = pl.ds(pl.multiple_of(which * half, half), half)
        wide = x.astype(F32)
        squares = jnp.sum(wide * wide, axis=1, keepdims=True)
        decay = dot(x, decay_wide[own, :])
        beta = lax.dot_general(x, strength[:, own], NT, preferred_element_type=F32)
        return squares, decay, beta[:, :heads]

    def project(x, which):
        own = pl.ds(pl.multiple_of(which * half, half), half)
        return [dot(x, weights[i, own, :]) for i in range(4)]

    def begin(m, span):
        own = pl.ds(pl.multiple_of(core * half, half), half)

        def first():
            x = gather(m, core, span)
            squares, decay, beta = glance(x, core)
            squares_own[span] = jnp.broadcast_to(squares, (size, width))
            decay_own[span] = decay
            beta_own[span] = beta

        def piece(i):
            acc[i, span] = dot(gather(m, core, span), weights[i, own, :])

        return [functools.partial(piece, 0), first] + [functools.partial(piece, i) for i in range(1, 4)]

    def chunk(m, span, keep, use, between):
        squares = squares_own[span, :1]
        decay = decay_own[span]
        beta = beta_own[span]
        for d in others:
            for h in range(heads):
                forward_copy(m, d, h, span).wait_recv()
            source = peer(group - d)
            x = gather(m, source, span)
            squares_other, decay_other, beta_other = glance(x, source)
            squares = squares + squares_other
            decay = decay + decay_other
            beta = beta + beta_other
            mats = project(x, source)
            if d < group - 1:
                for i in range(4):
                    acc[i, span] += mats[i]
        inv_rms = lax.rsqrt(squares / model_width + epsilon)

        row = lax.broadcasted_iota(jnp.int32, (size, lanes), 0)
        lane = lax.broadcasted_iota(jnp.int32, (size, lanes), 1)
        column = lane % size
        band = (lax.broadcasted_iota(jnp.int32, (8, lanes), 1) % size) // block

        beta = 1.0 / (1.0 + jnp.exp(-beta * inv_rms))
        pre = decay * inv_rms
        softplus = jnp.maximum(pre, 0.0) + jnp.log(1.0 + jnp.exp(-jnp.abs(pre)))
        log_decay = spike_wide[span, :] - speed_wide[...] * softplus
        lower = jnp.where(
            lax.broadcasted_iota(jnp.int32, (size, size), 0)
            >= lax.broadcasted_iota(jnp.int32, (size, size), 1),
            1.0,
            0.0,
        ).astype(BF16)
        high = log_decay.astype(BF16)
        rest = log_decay - high.astype(F32)
        after = jnp.concatenate([row > column] * groups, axis=1)

        def total(mask):
            picked = (jnp.where(after, a.astype(F32), 0.0) if mask else a for a in (high, rest))
            return sum(dot(lower, a) for a in picked)

        since = total(True)
        if use:
            whole = total(False)

        def packed(which, g):
            return jnp.concatenate([which[g + p * groups] for p in range(side)], axis=1)

        def apart(which, g):
            empty = jnp.zeros_like(which[0])
            return jnp.concatenate(
                [
                    jnp.concatenate(
                        [which[g + p * groups] if s == p else empty for s in range(side)], axis=1
                    )
                    for p in range(side)
                ],
                axis=0,
            )

        def stacked(square):
            if side == 1:
                return square
            return jnp.concatenate(
                [jnp.where(lane // size == p, square, jnp.zeros_like(square)) for p in range(side)],
                axis=0,
            )

        def columns(i, h):
            part = slice(h * width, (h + 1) * width)
            return (acc[i, span, part] + mats[i][:, part]) * inv_rms

        def norm(a):
            return lax.rsqrt(jnp.sum(a * a, axis=1, keepdims=True) + epsilon)

        keys = [silu(columns(0, h)) for h in range(heads)]
        rounded_keys = [a.astype(BF16) for a in keys]
        queries = [silu(columns(1, h)) for h in range(heads)]
        rounded_queries = [a.astype(BF16) for a in queries]
        gram = []
        for g in every:
            left = jnp.concatenate([packed(rounded_keys, g), packed(rounded_queries, g)], axis=0)
            gram.append(
                lax.dot_general(left, apart(rounded_keys, g), NT, preferred_element_type=F32)
            )
        key_scale = [norm(a) for a in keys]
        query_scale = [norm(a) * width ** (-0.5) for a in queries]
        force = [beta[:, h : h + 1] * key_scale[h] for h in range(heads)]
        weight = [force[h] * key_scale[h] for h in range(heads)]
        values = [silu(columns(2, h)) * force[h] for h in range(heads)]

        def stretch(parts, g):
            out = jnp.broadcast_to(parts[g], (size, lanes))
            for p in range(1, side):
                out = jnp.where(
                    lane >= p * size, jnp.broadcast_to(parts[g + p * groups], (size, lanes)), out
                )
            return out

        def section(wide, g):
            return wide[:, g * lanes : (g + 1) * lanes]

        decayed = [jnp.where(row >= column, jnp.exp(section(since, g)), 0.0) for g in every]
        scale = [stretch(weight, g) for g in every]
        system = [
            jnp.where(row > column, gram[g][:size] * decayed[g], 0.0) * scale[g] for g in every
        ]
        scores = [(gram[g][size:] * decayed[g]).astype(BF16) for g in every]

        before = None
        if use:
            past_keys = [past_key[h] for h in range(heads)]
            past_values = [past_value[h] for h in range(heads)]
            before = []
            for g in every:
                left = jnp.concatenate(
                    [packed(rounded_keys, g), packed(rounded_queries, g)], axis=0
                )
                cross = lax.dot_general(left, apart(past_keys, g), NT, preferred_element_type=F32)
                fade = jnp.exp(section(whole, g) + past_fade[g : g + 1, :])
                cross = (cross * jnp.concatenate([fade, fade], axis=0)).astype(BF16)
                before.append(
                    jnp.dot(cross, apart(past_values, g), preferred_element_type=F32)
                )
            for g in every:
                for p in range(side):
                    h = g + p * groups
                    part = slice(p * width, (p + 1) * width)
                    values[h] = values[h] - weight[h] * before[g][:size, part]

        tiles = block // 8
        inverse = []
        for g in every:
            compact = []
            for t in range(tiles):
                tile = system[g][t * 8 : t * 8 + 8]
                for r in range(1, pieces):
                    at = r * block + t * 8
                    tile = jnp.where(band == r, system[g][at : at + 8], tile)
                compact.append(tile)
            inner = lax.broadcasted_iota(jnp.int32, (8, lanes), 1) % block
            down_rows = lax.broadcasted_iota(jnp.int32, (8, lanes), 0)
            solved = [
                jnp.where(down_rows + t * 8 == inner, 1.0, 0.0).astype(F32) for t in range(tiles)
            ]
            start_of = lax.broadcasted_iota(jnp.int32, (8, lanes), 1) - inner
            for j in range(block - 1):
                source = jnp.broadcast_to(
                    solved[j // 8][j % 8 : j % 8 + 1, :], (8, lanes)
                )
                for t in range((j + 1) // 8, tiles):
                    factor = jnp.take_along_axis(
                        compact[t], start_of + j, axis=1, mode="promise_in_bounds"
                    )
                    solved[t] = solved[t] - factor * source
            inverse.append(
                jnp.concatenate(
                    [
                        jnp.where(band == r, solved[t], 0.0).astype(F32)
                        for r in range(pieces)
                        for t in range(tiles)
                    ],
                    axis=0,
                ).astype(BF16)
            )
        queue = between()

        def fill(count):
            for _ in range(min(count, len(queue))):
                queue.pop(0)()

        update = [dot(inverse[g], apart([a.astype(BF16) for a in values], g)) for g in every]

        def split(wide):
            return [
                wide[h % groups][:, (h // groups) * width : (h // groups + 1) * width].astype(BF16)
                for h in range(heads)
            ]

        if pieces > 1:
            outside = row // block != column // block
            chain = [
                dot(inverse[g], stacked(jnp.where(outside, system[g], 0.0).astype(BF16)))
                for g in every
            ]
            fill(2)
            sign = -1.0
            done = 1
            while done < pieces:
                rounded = [chain[g].astype(BF16) for g in every]
                current = split(update)
                update = [
                    update[g] + sign * dot(rounded[g], apart(current, g)) for g in every
                ]
                done *= 2
                sign = 1.0
                if done < pieces:
                    chain = [dot(rounded[g], stacked(rounded[g])) for g in every]
                fill(1)
        final = split(update)
        fill(1)
        mixed = [dot(scores[g], apart(final, g)) for g in every]
        fill(len(queue))
        if use:
            mixed = [mixed[g] + before[g][size:] for g in every]
        for h in range(heads):
            part = slice((h // groups) * width, (h // groups + 1) * width)
            raw = mixed[h % groups][:, part]
            gate = silu(columns(3, h)) * gain[:, h * width : (h + 1) * width]
            mean = jnp.mean(raw * raw, axis=1, keepdims=True)
            unit = query_scale[h]
            head_out = raw * (unit * lax.rsqrt(unit * unit * mean + epsilon)) * gate
            x = xin[m, core * heads + h, span].astype(F32)
            xout[m, h, span] = (x + head_out.astype(BF16).astype(F32)).astype(BF16)
        if keep:
            for h in range(heads):
                past_key[h] = rounded_keys[h]
                past_value[h] = final[h]
            for g in every:
                past_fade[g : g + 1, :] = section(since, g)[size - 1 : size, :]

    def arrive(m, span):
        for h in range(heads):
            next_copy(m, h, span).wait_recv()
            for d in others:
                forward_copy(m, d, h, span).start()

    def leave(m, span):
        @pl.when(stage < last)
        def _():
            for h in range(heads):
                next_copy(m, h, span).start()

        @pl.when((stage == last) & (m < last))
        def _():
            for h in range(heads):
                exit_copy(m, h, span).start()

    def step(m, _):
        for i, span in enumerate(spans):

            def between(i=i):
                if i + 1 < len(spans):
                    following, ahead = m, spans[i + 1]

                    @pl.when((stage > 0) | (m > 0))
                    def _():
                        arrive(following, ahead)

                else:
                    following, ahead = lax.rem(m + 1, stages), spans[0]

                    @pl.when(m < last)
                    def _():
                        arrive(following, ahead)

                return begin(following, ahead)

            chunk(m, span, keep=i + 1 < len(spans), use=i > 0, between=between)
            leave(m, span)
        return 0

    @pl.when(stage > 1)
    def _():
        pl.semaphore_wait(go_sem, 1)
        for span in spans:
            for h in range(heads):
                entry_copy(h, span).start()

    @pl.when(stage == 1)
    def _():
        entry_copy(1, spans[0]).wait_send()

    @pl.when(stage > 1)
    def _():
        entry_copy(1, spans[-1]).wait_send()

    @pl.when((stage > 0) & (stage < last))
    def _():
        pl.semaphore_signal(go_sem, inc=1, device_id={"pp": stage + 1}, device_id_type=MESH)

    @pl.when(stage > 0)
    def _():
        arrive(0, spans[0])

    for load in loads:
        load.wait()
    for piece in begin(0, spans[0]):
        piece()

    lax.fori_loop(0, stages, step, 0)

    @pl.when(stage == last)
    def _():
        for h in range(heads):
            yin[h] = xout[last, h]

    def part_copy(d, span):
        at = span.start // size
        return pltpu.make_async_remote_copy(
            src_ref=part_mine.at[span],
            dst_ref=part_other.at[d - 1, span],
            send_sem=part_send.at[d - 1, at],
            recv_sem=part_recv.at[d - 1, at],
            device_id={"tp": peer(d)},
            device_id_type=MESH,
        )

    for span in spans:

        @pl.when(stage < last)
        def _(span=span):
            for h in range(heads):
                exit_copy(0, h, span).wait_recv()

        final = [yin[h, span].astype(F32) for h in range(heads)]
        total = sum(a * a for a in final)
        total = jnp.sum(total, axis=1, keepdims=True)
        part_mine[span] = jnp.broadcast_to(total, (size, width))
        for d in others:
            part_copy(d, span).start()

    @pl.when(stage > 0)
    def _():
        for span in spans:
            for h in range(heads):
                f1 = h == 1 and span is spans[0]
                f2 = h == 1 and span is spans[-1]
                wanted = (not f1) if f1 == f2 else (jnp.where(stage == 1, int(not f1), int(not f2)) == 1)

                @pl.when(wanted)
                def _(h=h, span=span):
                    entry_copy(h, span).wait_send()

    def drain(m, _):
        for span in spans:
            for h in range(heads):
                for d in others:
                    forward_copy(m, d, h, span).wait_send()

        @pl.when((stage < last) | (m < last))
        def _():
            for span in spans:
                for h in range(heads):
                    next_copy(m, h, span).wait_send()

        return 0

    lax.fori_loop(0, stages, drain, 0)
    for span in spans:
        total = part_mine[span]
        for d in others:
            part_copy(d, span).wait()
            total = total + part_other[d - 1, span]
        inv_rms = lax.rsqrt(total / model_width + epsilon)
        for h in range(heads):
            part = slice(h * width, (h + 1) * width)
            scaled = yin[h, span].astype(F32) * inv_rms * closing_gain[:, part]
            out[span, part] = scaled.astype(BF16)


def on_device(
    stages,
    group,
    tokens,
    query_matrix,
    key_matrix,
    value_matrix,
    output_gate_weight,
    strength_weight,
    decay_input_weight,
    decay_scale_table,
    log_spike_decay,
    head_norm_gain,
    closing_norm_gain,
):
    _, length, half = tokens.shape
    heads = strength_weight.shape[-1]
    width = half // heads
    parts = 2 if heads % 2 == 0 else 1
    size = length // parts

    def rows_of(weight):
        return jnp.pad(weight[0].T, ((0, 1), (0, 0))) if heads == 1 else weight[0].T

    vmem = pl.BlockSpec(memory_space=pltpu.VMEM)
    anywhere = pl.BlockSpec(memory_space=pltpu.HBM)
    dma = pltpu.SemaphoreType.DMA
    result = pl.pallas_call(
        functools.partial(stack_kernel, stages, group, size),
        out_shape=pltpu.VMEM((length, half), BF16),
        in_specs=[anywhere] * 11,
        out_specs=vmem,
        scratch_shapes=[
            pltpu.VMEM((max(heads, 2), group * half), BF16),
            pltpu.VMEM((max(heads, 2), group * half), BF16),
            pltpu.VMEM((1, heads), F32),
            pltpu.VMEM((heads, length), F32),
            pltpu.VMEM((1, half), F32),
            pltpu.VMEM((1, half), F32),
            pltpu.VMEM((4, group * half, half), BF16),
            pltpu.VMEM((4, length, half), F32),
            pltpu.VMEM((length, width), F32),
            pltpu.VMEM((length, heads), F32),
            pltpu.VMEM((length, heads * size), F32),
            pltpu.VMEM((group * half, heads * size), BF16),
            pltpu.VMEM((1, heads * size), F32),
            pltpu.VMEM((length, heads * size), F32),
            pltpu.VMEM((stages, group * heads, length, width), BF16),
            pltpu.VMEM((stages + 1, heads, length, width), BF16),
            pltpu.VMEM((heads, length, width), BF16),
            pltpu.VMEM((heads, size, width), BF16),
            pltpu.VMEM((heads, size, width), BF16),
            pltpu.VMEM((8, length), F32),
            pltpu.VMEM((length, width), F32),
            pltpu.VMEM((group - 1, length, width), F32),
            dma((4,)),
            dma((6,)),
            dma((heads,)),
            pltpu.SemaphoreType.REGULAR,
            dma((stages, parts, heads)),
            dma((parts, heads)),
            dma((stages, group - 1, parts, heads)),
            dma((stages, group - 1, parts, heads)),
            dma((stages, parts, heads)),
            dma((parts, heads)),
            dma((group - 1, parts)),
            dma((group - 1, parts)),
        ],
        compiler_params=pltpu.CompilerParams(
            collective_id=0, has_side_effects=True, vmem_limit_bytes=60 * 1024 * 1024
        ),
    )(
        tokens[0],
        query_matrix[0],
        key_matrix[0],
        value_matrix[0],
        output_gate_weight[0],
        rows_of(strength_weight),
        rows_of(decay_input_weight),
        decay_scale_table,
        log_spike_decay[0].T,
        head_norm_gain,
        closing_norm_gain[None],
    )
    return result[None]


def solution(mesh):
    placed = (
        P("pp", "fs", "tp"),
        P("pp", None, "tp"),
        P("pp", None, "tp"),
        P("pp", None, "tp"),
        P("pp", None, "tp"),
        P("pp", None, "tp"),
        P("pp", None, "tp"),
        P("pp", "tp"),
        P("pp", None, "tp"),
        P("pp", "tp"),
        P("tp"),
    )
    return jax.shard_map(
        functools.partial(on_device, mesh.shape["pp"], mesh.shape["tp"]),
        mesh=mesh,
        in_specs=placed,
        out_specs=P("pp", "fs", "tp"),
        check_vma=False,
    )
```

```python
import functools
import jax
import jax.numpy as jnp
from jax import lax
from jax.experimental import pallas as pl
from jax.experimental.pallas import tpu as pltpu
from jax.sharding import PartitionSpec as P

epsilon = 1e-06
F32 = jnp.float32
BF16 = jnp.bfloat16
MESH = pl.DeviceIdType.MESH
NT = (((1,), (1,)), ((), ()))


def silu(a):
    return a * (0.5 + 0.5 * jnp.tanh(0.5 * a))


def dot(a, b):
    return jnp.dot(a.astype(BF16), b.astype(BF16), preferred_element_type=F32)


def stack_kernel(
    stages,
    group,
    size,
    tokens,
    query_hbm,
    key_hbm,
    value_hbm,
    gate_hbm,
    strength_hbm,
    decay_in_hbm,
    decay_speed_hbm,
    spike_hbm,
    gain_hbm,
    closing_hbm,
    out,
    strength,
    decay_in,
    decay_speed,
    spike,
    gain,
    closing_gain,
    weights,
    acc,
    squares_own,
    beta_own,
    decay_own,
    decay_wide,
    speed_wide,
    spike_wide,
    xin,
    xout,
    yin,
    past_key,
    past_value,
    past_fade,
    part_exit,
    part_mine,
    part_other,
    w_sem,
    small_sem,
    token_sem,
    go_sem,
    in_sem,
    entry_sem,
    fwd_send,
    fwd_recv,
    out_send,
    y_recv,
    part_send,
    part_recv,
    exit_sem,
):
    stage = lax.axis_index("pp")
    core = lax.axis_index("tp")
    last = stages - 1
    length, half = tokens.shape
    heads = xout.shape[1]
    width = half // heads
    model_width = group * half
    others = range(1, group)
    spans = [slice(start, start + size) for start in range(0, length, size)]

    def peer(d):
        return lax.rem(core + d, group)

    barrier = pltpu.get_barrier_semaphore()

    @pl.when(stage > 0)
    def _():
        pl.semaphore_signal(barrier, inc=1, device_id={"pp": stage - 1}, device_id_type=MESH)

    @pl.when(stage < last)
    def _():
        pl.semaphore_signal(barrier, inc=1, device_id={"pp": stage + 1}, device_id_type=MESH)

    for d in others:
        pl.semaphore_signal(barrier, inc=1, device_id={"tp": peer(d)}, device_id_type=MESH)

    def token_copy(h, target):
        return pltpu.make_async_copy(
            tokens.at[:, h * width : (h + 1) * width], target, token_sem.at[h]
        )

    @pl.when(stage == 0)
    def _():
        for h in range(heads):
            token_copy(h, xin.at[0, core * heads + h]).start()

    @pl.when(stage > 0)
    def _():
        for h in range(heads):
            token_copy(h, xout.at[stages, h]).start()

    small_loads = [
        pltpu.make_async_copy(a, b, small_sem.at[i])
        for i, (a, b) in enumerate(
            (
                (strength_hbm, strength),
                (decay_in_hbm, decay_in),
                (decay_speed_hbm, decay_speed),
                (spike_hbm, spike),
                (gain_hbm, gain),
                (closing_hbm, closing_gain),
            )
        )
    ]
    for load in small_loads:
        load.start()
    loads = [
        pltpu.make_async_copy(ref, weights.at[i], w_sem.at[i])
        for i, ref in enumerate((key_hbm, query_hbm, value_hbm, gate_hbm))
    ]
    for load in loads:
        load.start()

    def entry_copy(h, span):
        return pltpu.make_async_remote_copy(
            src_ref=xout.at[stages, h, span],
            dst_ref=xin.at[stage, core * heads + h, span],
            send_sem=entry_sem.at[span.start // size, h],
            recv_sem=in_sem.at[stage, span.start // size, h],
            device_id={"pp": 0},
            device_id_type=MESH,
        )

    def next_copy(m, h, span):
        return pltpu.make_async_remote_copy(
            src_ref=xout.at[m, h, span],
            dst_ref=xin.at[m, core * heads + h, span],
            send_sem=out_send.at[m, span.start // size, h],
            recv_sem=in_sem.at[m, span.start // size, h],
            device_id={"pp": lax.rem(stage + 1, stages)},
            device_id_type=MESH,
        )

    def exit_copy(m, h, span):
        return pltpu.make_async_remote_copy(
            src_ref=xout.at[m, h, span],
            dst_ref=yin.at[h, span],
            send_sem=out_send.at[m, span.start // size, h],
            recv_sem=y_recv.at[span.start // size, h],
            device_id={"pp": m},
            device_id_type=MESH,
        )

    def forward_copy(m, d, h, span):
        return pltpu.make_async_remote_copy(
            src_ref=xin.at[m, core * heads + h, span],
            dst_ref=xin.at[m, core * heads + h, span],
            send_sem=fwd_send.at[m, d - 1, span.start // size, h],
            recv_sem=fwd_recv.at[m, d - 1, span.start // size, h],
            device_id={"tp": peer(d)},
            device_id_type=MESH,
        )

    for h in range(heads):
        token_copy(h, xout.at[stages, h]).wait()
    pl.semaphore_wait(
        barrier, group - 1 + (stage > 0).astype(jnp.int32) + (stage < last).astype(jnp.int32)
    )

    @pl.when(stage == 0)
    def _():
        for span in spans:
            for h in range(heads):
                for d in others:
                    forward_copy(0, d, h, span).start()

    @pl.when(stage == 1)
    def _():
        for span in spans:
            for h in range(heads):
                entry_copy(h, span).start()

    for load in small_loads:
        load.wait()
    side = min(length // size, heads)
    groups = heads // side
    lanes = side * size
    block = min(16, size)
    pieces = size // block
    every = range(groups)
    spike_columns = jnp.concatenate(
        [spike[...], jnp.zeros((length - heads, length), F32)], axis=0
    ).T
    for g in every:
        for p in range(side):
            h = g + p * groups
            at = slice(g * lanes + p * size, g * lanes + (p + 1) * size)
            speed_wide[:, at] = jnp.broadcast_to(decay_speed[:, h : h + 1], (1, size))
        spread = jnp.broadcast_to(spike_columns[:, g : g + 1], (length, lanes))
        for p in range(1, side):
            h = g + p * groups
            lane = lax.broadcasted_iota(jnp.int32, (length, lanes), 1)
            other = jnp.broadcast_to(spike_columns[:, h : h + 1], (length, lanes))
            spread = jnp.where(lane >= p * size, other, spread)
        spike_wide[:, g * lanes : (g + 1) * lanes] = spread
    tile = min(256, model_width)
    same = lax.broadcasted_iota(jnp.int32, (tile, tile), 0) == lax.broadcasted_iota(
        jnp.int32, (tile, tile), 1
    )
    identity = jnp.where(same, 1.0, 0.0).astype(BF16)
    for start in range(0, model_width, tile):
        part = decay_in[:heads, start : start + tile].astype(F32)
        wide = jnp.concatenate(
            [
                jnp.broadcast_to(part[g + p * groups : g + p * groups + 1], (size, tile))
                for g in every
                for p in range(side)
            ],
            axis=0,
        ).astype(BF16)
        decay_wide[start : start + tile, :] = lax.dot_general(
            identity, wide, NT, preferred_element_type=F32
        ).astype(BF16)

    def gather(m, which, span):
        return jnp.concatenate([xin[m, which * heads + h, span] for h in range(heads)], axis=1)

    def glance(x, which):
        own = pl.ds(pl.multiple_of(which * half, half), half)
        wide = x.astype(F32)
        squares = jnp.sum(wide * wide, axis=1, keepdims=True)
        decay = dot(x, decay_wide[own, :])
        beta = lax.dot_general(x, strength[:, own], NT, preferred_element_type=F32)
        return squares, decay, beta[:, :heads]

    def project(x, which):
        own = pl.ds(pl.multiple_of(which * half, half), half)
        return [dot(x, weights[i, own, :]) for i in range(4)]

    def begin(m, span):
        own = pl.ds(pl.multiple_of(core * half, half), half)

        def first():
            x = gather(m, core, span)
            squares, decay, beta = glance(x, core)
            squares_own[span] = jnp.broadcast_to(squares, (size, width))
            decay_own[span] = decay
            beta_own[span] = beta

        def piece(i):
            acc[i, span] = dot(gather(m, core, span), weights[i, own, :])

        return [functools.partial(piece, 0), first] + [functools.partial(piece, i) for i in range(1, 4)]

    def chunk(m, span, keep, use, between):
        squares = squares_own[span, :1]
        decay = decay_own[span]
        beta = beta_own[span]
        for d in others:
            for h in range(heads):
                forward_copy(m, d, h, span).wait_recv()
            source = peer(group - d)
            x = gather(m, source, span)
            squares_other, decay_other, beta_other = glance(x, source)
            squares = squares + squares_other
            decay = decay + decay_other
            beta = beta + beta_other
            mats = project(x, source)
            if d < group - 1:
                for i in range(4):
                    acc[i, span] += mats[i]
        inv_rms = lax.rsqrt(squares / model_width + epsilon)

        row = lax.broadcasted_iota(jnp.int32, (size, lanes), 0)
        lane = lax.broadcasted_iota(jnp.int32, (size, lanes), 1)
        column = lane % size
        band = (lax.broadcasted_iota(jnp.int32, (8, lanes), 1) % size) // block

        beta = 1.0 / (1.0 + jnp.exp(-beta * inv_rms))
        pre = decay * inv_rms
        softplus = jnp.maximum(pre, 0.0) + jnp.log(1.0 + jnp.exp(-jnp.abs(pre)))
        log_decay = spike_wide[span, :] - speed_wide[...] * softplus
        lower = jnp.where(
            lax.broadcasted_iota(jnp.int32, (size, size), 0)
            >= lax.broadcasted_iota(jnp.int32, (size, size), 1),
            1.0,
            0.0,
        ).astype(BF16)
        high = log_decay.astype(BF16)
        rest = log_decay - high.astype(F32)
        after = jnp.concatenate([row > column] * groups, axis=1)

        def total(mask):
            picked = (jnp.where(after, a.astype(F32), 0.0) if mask else a for a in (high, rest))
            return sum(dot(lower, a) for a in picked)

        since = total(True)
        if use:
            whole = total(False)

        def packed(which, g):
            return jnp.concatenate([which[g + p * groups] for p in range(side)], axis=1)

        def apart(which, g):
            empty = jnp.zeros_like(which[0])
            return jnp.concatenate(
                [
                    jnp.concatenate(
                        [which[g + p * groups] if s == p else empty for s in range(side)], axis=1
                    )
                    for p in range(side)
                ],
                axis=0,
            )

        def stacked(square):
            if side == 1:
                return square
            return jnp.concatenate(
                [jnp.where(lane // size == p, square, jnp.zeros_like(square)) for p in range(side)],
                axis=0,
            )

        def columns(i, h):
            part = slice(h * width, (h + 1) * width)
            return (acc[i, span, part] + mats[i][:, part]) * inv_rms

        def norm(a):
            return lax.rsqrt(jnp.sum(a * a, axis=1, keepdims=True) + epsilon)

        keys = [silu(columns(0, h)) for h in range(heads)]
        rounded_keys = [a.astype(BF16) for a in keys]
        queries = [silu(columns(1, h)) for h in range(heads)]
        rounded_queries = [a.astype(BF16) for a in queries]
        gram = []
        for g in every:
            left = jnp.concatenate([packed(rounded_keys, g), packed(rounded_queries, g)], axis=0)
            gram.append(
                lax.dot_general(left, apart(rounded_keys, g), NT, preferred_element_type=F32)
            )
        key_scale = [norm(a) for a in keys]
        query_scale = [norm(a) * width ** (-0.5) for a in queries]
        force = [beta[:, h : h + 1] * key_scale[h] for h in range(heads)]
        weight = [force[h] * key_scale[h] for h in range(heads)]
        values = [silu(columns(2, h)) * force[h] for h in range(heads)]

        def stretch(parts, g):
            out = jnp.broadcast_to(parts[g], (size, lanes))
            for p in range(1, side):
                out = jnp.where(
                    lane >= p * size, jnp.broadcast_to(parts[g + p * groups], (size, lanes)), out
                )
            return out

        def section(wide, g):
            return wide[:, g * lanes : (g + 1) * lanes]

        decayed = [jnp.where(row >= column, jnp.exp(section(since, g)), 0.0) for g in every]
        scale = [stretch(weight, g) for g in every]
        system = [
            jnp.where(row > column, gram[g][:size] * decayed[g], 0.0) * scale[g] for g in every
        ]
        scores = [(gram[g][size:] * decayed[g]).astype(BF16) for g in every]

        before = None
        if use:
            past_keys = [past_key[h] for h in range(heads)]
            past_values = [past_value[h] for h in range(heads)]
            before = []
            for g in every:
                left = jnp.concatenate(
                    [packed(rounded_keys, g), packed(rounded_queries, g)], axis=0
                )
                cross = lax.dot_general(left, apart(past_keys, g), NT, preferred_element_type=F32)
                fade = jnp.exp(section(whole, g) + past_fade[g : g + 1, :])
                cross = (cross * jnp.concatenate([fade, fade], axis=0)).astype(BF16)
                before.append(
                    jnp.dot(cross, apart(past_values, g), preferred_element_type=F32)
                )
            for g in every:
                for p in range(side):
                    h = g + p * groups
                    part = slice(p * width, (p + 1) * width)
                    values[h] = values[h] - weight[h] * before[g][:size, part]

        tiles = block // 8
        inverse = []
        for g in every:
            compact = []
            for t in range(tiles):
                tile = system[g][t * 8 : t * 8 + 8]
                for r in range(1, pieces):
                    at = r * block + t * 8
                    tile = jnp.where(band == r, system[g][at : at + 8], tile)
                compact.append(tile)
            inner = lax.broadcasted_iota(jnp.int32, (8, lanes), 1) % block
            down_rows = lax.broadcasted_iota(jnp.int32, (8, lanes), 0)
            solved = [
                jnp.where(down_rows + t * 8 == inner, 1.0, 0.0).astype(F32) for t in range(tiles)
            ]
            start_of = lax.broadcasted_iota(jnp.int32, (8, lanes), 1) - inner
            for j in range(block - 1):
                source = jnp.broadcast_to(
                    solved[j // 8][j % 8 : j % 8 + 1, :], (8, lanes)
                )
                for t in range((j + 1) // 8, tiles):
                    factor = jnp.take_along_axis(
                        compact[t], start_of + j, axis=1, mode="promise_in_bounds"
                    )
                    solved[t] = solved[t] - factor * source
            inverse.append(
                jnp.concatenate(
                    [
                        jnp.where(band == r, solved[t], 0.0).astype(F32)
                        for r in range(pieces)
                        for t in range(tiles)
                    ],
                    axis=0,
                ).astype(BF16)
            )
        queue = between()

        def fill(count):
            for _ in range(min(count, len(queue))):
                queue.pop(0)()

        update = [dot(inverse[g], apart([a.astype(BF16) for a in values], g)) for g in every]

        def split(wide):
            return [
                wide[h % groups][:, (h // groups) * width : (h // groups + 1) * width].astype(BF16)
                for h in range(heads)
            ]

        if pieces > 1:
            outside = row // block != column // block
            chain = [
                dot(inverse[g], stacked(jnp.where(outside, system[g], 0.0).astype(BF16)))
                for g in every
            ]
            fill(2)
            sign = -1.0
            done = 1
            while done < pieces:
                rounded = [chain[g].astype(BF16) for g in every]
                current = split(update)
                update = [
                    update[g] + sign * dot(rounded[g], apart(current, g)) for g in every
                ]
                done *= 2
                sign = 1.0
                if done < pieces:
                    chain = [dot(rounded[g], stacked(rounded[g])) for g in every]
                fill(1)
        final = split(update)
        fill(1)
        mixed = [dot(scores[g], apart(final, g)) for g in every]
        fill(len(queue))
        if use:
            mixed = [mixed[g] + before[g][size:] for g in every]
        for h in range(heads):
            part = slice((h // groups) * width, (h // groups + 1) * width)
            raw = mixed[h % groups][:, part]
            gate = silu(columns(3, h)) * gain[:, h * width : (h + 1) * width]
            mean = jnp.mean(raw * raw, axis=1, keepdims=True)
            unit = query_scale[h]
            head_out = raw * (unit * lax.rsqrt(unit * unit * mean + epsilon)) * gate
            x = xin[m, core * heads + h, span].astype(F32)
            xout[m, h, span] = (x + head_out.astype(BF16).astype(F32)).astype(BF16)
        if keep:
            for h in range(heads):
                past_key[h] = rounded_keys[h]
                past_value[h] = final[h]
            for g in every:
                past_fade[g : g + 1, :] = section(since, g)[size - 1 : size, :]

    def arrive(m, span):
        for h in range(heads):
            next_copy(m, h, span).wait_recv()
            for d in others:
                forward_copy(m, d, h, span).start()

    def exit_part(d):
        return pltpu.make_async_remote_copy(
            src_ref=part_exit,
            dst_ref=part_other.at[d - 1, spans[-1]],
            send_sem=exit_sem.at[d - 1],
            recv_sem=part_recv.at[d - 1, len(spans) - 1],
            device_id={"pp": last - 1, "tp": peer(d)},
            device_id_type=MESH,
        )

    def leave(m, span):
        @pl.when(stage < last)
        def _():
            for h in range(heads):
                next_copy(m, h, span).start()

        @pl.when((stage == last) & (m < last))
        def _():
            for h in range(heads):
                exit_copy(m, h, span).start()

    def step(m, _):
        for i, span in enumerate(spans):

            def between(i=i):
                if i + 1 < len(spans):
                    following, ahead = m, spans[i + 1]

                    @pl.when((stage > 0) | (m > 0))
                    def _():
                        arrive(following, ahead)

                else:
                    following, ahead = lax.rem(m + 1, stages), spans[0]

                    @pl.when(m < last)
                    def _():
                        arrive(following, ahead)

                return begin(following, ahead)

            chunk(m, span, keep=i + 1 < len(spans), use=i > 0, between=between)
            leave(m, span)

            if i + 1 == len(spans):

                @pl.when((stage == last) & (m == last - 1))
                def _(span=span):
                    rows = [xout[m, h, span].astype(F32) for h in range(heads)]
                    total = jnp.sum(sum(a * a for a in rows), axis=1, keepdims=True)
                    part_exit[...] = jnp.broadcast_to(total, (size, width))
                    for d in others:
                        exit_part(d).start()

        return 0

    @pl.when(stage > 1)
    def _():
        pl.semaphore_wait(go_sem, 1)
        for span in spans:
            for h in range(heads):
                entry_copy(h, span).start()

    @pl.when(stage == 1)
    def _():
        entry_copy(1, spans[0]).wait_send()

    @pl.when(stage > 1)
    def _():
        entry_copy(1, spans[-1]).wait_send()

    @pl.when((stage > 0) & (stage < last))
    def _():
        pl.semaphore_signal(go_sem, inc=1, device_id={"pp": stage + 1}, device_id_type=MESH)

    @pl.when(stage > 0)
    def _():
        arrive(0, spans[0])

    for load in loads:
        load.wait()
    for piece in begin(0, spans[0]):
        piece()

    lax.fori_loop(0, stages, step, 0)

    @pl.when(stage == last)
    def _():
        for h in range(heads):
            yin[h] = xout[last, h]

    def part_copy(d, span):
        at = span.start // size
        return pltpu.make_async_remote_copy(
            src_ref=part_mine.at[span],
            dst_ref=part_other.at[d - 1, span],
            send_sem=part_send.at[d - 1, at],
            recv_sem=part_recv.at[d - 1, at],
            device_id={"tp": peer(d)},
            device_id_type=MESH,
        )

    for span in spans:

        @pl.when(stage < last)
        def _(span=span):
            for h in range(heads):
                exit_copy(0, h, span).wait_recv()

        final = [yin[h, span].astype(F32) for h in range(heads)]
        total = sum(a * a for a in final)
        total = jnp.sum(total, axis=1, keepdims=True)
        part_mine[span] = jnp.broadcast_to(total, (size, width))
        told = (stage == last - 1) if span is spans[-1] else (stage < 0)

        @pl.when(jnp.logical_not(told))
        def _(span=span):
            for d in others:
                part_copy(d, span).start()

    @pl.when(stage > 0)
    def _():
        for span in spans:
            for h in range(heads):
                f1 = h == 1 and span is spans[0]
                f2 = h == 1 and span is spans[-1]
                wanted = (not f1) if f1 == f2 else (jnp.where(stage == 1, int(not f1), int(not f2)) == 1)

                @pl.when(wanted)
                def _(h=h, span=span):
                    entry_copy(h, span).wait_send()

    def drain(m, _):
        for span in spans:
            for h in range(heads):
                for d in others:
                    forward_copy(m, d, h, span).wait_send()

        @pl.when((stage < last) | (m < last))
        def _():
            for span in spans:
                for h in range(heads):
                    next_copy(m, h, span).wait_send()

        return 0

    lax.fori_loop(0, stages, drain, 0)
    @pl.when(stage == last)
    def _():
        for d in others:
            exit_part(d).wait_send()

    for span in spans:
        told = (stage == last - 1) if span is spans[-1] else (stage < 0)

        @pl.when(jnp.logical_not(told))
        def _(span=span):
            for d in others:
                part_copy(d, span).wait_send()

    for span in spans:
        total = part_mine[span]
        for d in others:
            part_copy(d, span).wait_recv()
            total = total + part_other[d - 1, span]
        inv_rms = lax.rsqrt(total / model_width + epsilon)
        for h in range(heads):
            part = slice(h * width, (h + 1) * width)
            scaled = yin[h, span].astype(F32) * inv_rms * closing_gain[:, part]
            out[span, part] = scaled.astype(BF16)


def on_device(
    stages,
    group,
    tokens,
    query_matrix,
    key_matrix,
    value_matrix,
    output_gate_weight,
    strength_weight,
    decay_input_weight,
    decay_scale_table,
    log_spike_decay,
    head_norm_gain,
    closing_norm_gain,
):
    _, length, half = tokens.shape
    heads = strength_weight.shape[-1]
    width = half // heads
    parts = 2 if heads % 2 == 0 else 1
    size = length // parts

    def rows_of(weight):
        return jnp.pad(weight[0].T, ((0, 1), (0, 0))) if heads == 1 else weight[0].T

    vmem = pl.BlockSpec(memory_space=pltpu.VMEM)
    anywhere = pl.BlockSpec(memory_space=pltpu.HBM)
    dma = pltpu.SemaphoreType.DMA
    result = pl.pallas_call(
        functools.partial(stack_kernel, stages, group, size),
        out_shape=pltpu.VMEM((length, half), BF16),
        in_specs=[anywhere] * 11,
        out_specs=vmem,
        scratch_shapes=[
            pltpu.VMEM((max(heads, 2), group * half), BF16),
            pltpu.VMEM((max(heads, 2), group * half), BF16),
            pltpu.VMEM((1, heads), F32),
            pltpu.VMEM((heads, length), F32),
            pltpu.VMEM((1, half), F32),
            pltpu.VMEM((1, half), F32),
            pltpu.VMEM((4, group * half, half), BF16),
            pltpu.VMEM((4, length, half), F32),
            pltpu.VMEM((length, width), F32),
            pltpu.VMEM((length, heads), F32),
            pltpu.VMEM((length, heads * size), F32),
            pltpu.VMEM((group * half, heads * size), BF16),
            pltpu.VMEM((1, heads * size), F32),
            pltpu.VMEM((length, heads * size), F32),
            pltpu.VMEM((stages, group * heads, length, width), BF16),
            pltpu.VMEM((stages + 1, heads, length, width), BF16),
            pltpu.VMEM((heads, length, width), BF16),
            pltpu.VMEM((heads, size, width), BF16),
            pltpu.VMEM((heads, size, width), BF16),
            pltpu.VMEM((8, length), F32),
            pltpu.VMEM((size, width), F32),
            pltpu.VMEM((length, width), F32),
            pltpu.VMEM((group - 1, length, width), F32),
            dma((4,)),
            dma((6,)),
            dma((heads,)),
            pltpu.SemaphoreType.REGULAR,
            dma((stages, parts, heads)),
            dma((parts, heads)),
            dma((stages, group - 1, parts, heads)),
            dma((stages, group - 1, parts, heads)),
            dma((stages, parts, heads)),
            dma((parts, heads)),
            dma((group - 1, parts)),
            dma((group - 1, parts)),
            dma((group - 1,)),
        ],
        compiler_params=pltpu.CompilerParams(
            collective_id=0, has_side_effects=True, vmem_limit_bytes=60 * 1024 * 1024
        ),
    )(
        tokens[0],
        query_matrix[0],
        key_matrix[0],
        value_matrix[0],
        output_gate_weight[0],
        rows_of(strength_weight),
        rows_of(decay_input_weight),
        decay_scale_table,
        log_spike_decay[0].T,
        head_norm_gain,
        closing_norm_gain[None],
    )
    return result[None]


def solution(mesh):
    placed = (
        P("pp", "fs", "tp"),
        P("pp", None, "tp"),
        P("pp", None, "tp"),
        P("pp", None, "tp"),
        P("pp", None, "tp"),
        P("pp", None, "tp"),
        P("pp", None, "tp"),
        P("pp", "tp"),
        P("pp", None, "tp"),
        P("pp", "tp"),
        P("tp"),
    )
    return jax.shard_map(
        functools.partial(on_device, mesh.shape["pp"], mesh.shape["tp"]),
        mesh=mesh,
        in_specs=placed,
        out_specs=P("pp", "fs", "tp"),
        check_vma=False,
    )
```
